32 devices in a mesh: fs: 8 (over z, x), tp: 4 (over y, core).
Axes of the slice: x: 2, y: 2, z: 4, core: 2. Of those that a mesh axis runs over, the one named last changes fastest.
Arguments:
- tokens: bfloat16 [4096, 2048], P(('fs', 'tp')), may hold values from -6 to 6
- gate_weight: bfloat16 [2048, 6144], P('fs', 'tp'), may hold values from -0.125 to 0.125
- value_weight: bfloat16 [2048, 6144], P('fs', 'tp'), may hold values from -0.125 to 0.125
- gate_taps: float32 [3, 6144], P(None, 'tp'), may hold values from -3.5 to 3.5
- value_taps: float32 [3, 6144], P(None, 'tp'), may hold values from -3.5 to 3.5
- down_weight: bfloat16 [6144, 2048], P('tp', 'fs'), may hold values from -0.078125 to 0.078125
- norm_gain: float32 [2048], replicated, may hold values from 0.1 to 1.9
- norm_shift: float32 [2048], replicated, may hold values from -3 to 3
Outputs:
- mixed: bfloat16 [4096, 2048], P(('fs', 'tp'))
The draws below stay inside these ranges and needn't reach their ends.
All inputs are finite; a program needn't handle non-finite values.
Results may differ from the reference program's by a relative error of at most 0.017.
Values may be sent and summed in bfloat16 or wider, within the bound.
A program may use at most 256 MiB of HBM per device.

```python
import jax
import jax.numpy as jnp
from jax import lax

D = 2048
FF = 6144
TAPS = 3
TOK_DEV = 128
TOKENS = 4096
N_FS = 8
N_TP = 4


def block_scale(own_key, shape, cuts, smallest, top_value):
    level = 1.0
    for position, blocks in cuts:
        draws = jax.random.uniform(jax.random.fold_in(jax.random.fold_in(own_key, 6), position), (blocks,), jnp.float32, smallest / len(cuts), top_value / len(cuts))
        level = level * jnp.repeat(jnp.exp(draws), shape[position] // blocks).reshape((-1,) + (1,) * (len(shape) - 1 - position))
    return level


def bell_draw(stream_key, shape, width, reach, shards=(), dtype=jnp.bfloat16):
    array = width * jax.random.normal(stream_key, shape, jnp.float32)
    if shards:
        array = array * block_scale(stream_key, shape, shards, -0.22, 0.18)
    return jnp.clip(array, -reach, reach).astype(dtype)


def setup_inputs(seed: int = 0) -> dict:
    arg_keys = jax.random.split(jax.random.key(seed), 9)
    tokens = bell_draw(arg_keys[0], (TOKENS, D), 1.0, 6.0, ((0, 32),))
    gate_weight = bell_draw(arg_keys[1], (D, FF), D ** -0.5, 0.125, ((0, 8), (1, 4)))
    value_weight = bell_draw(arg_keys[2], (D, FF), D ** -0.5, 0.125, ((0, 8), (1, 4)))
    gate_taps = bell_draw(arg_keys[3], (TAPS, FF), TAPS ** -0.5, 3.5, ((1, 4),), jnp.float32)
    value_taps = bell_draw(arg_keys[4], (TAPS, FF), TAPS ** -0.5, 3.5, ((1, 4),), jnp.float32)
    down_weight = bell_draw(arg_keys[5], (FF, D), FF ** -0.5, 0.078125, ((0, 4), (1, 8)))
    norm_gain = jnp.clip(1.0 + 0.18 * jax.random.normal(arg_keys[6], (D,), jnp.float32), 0.1, 1.9)
    norm_shift = bell_draw(arg_keys[7], (D,), 0.5, 3.0, (), jnp.float32)
    return dict(tokens=tokens, gate_weight=gate_weight, value_weight=value_weight, gate_taps=gate_taps, value_taps=value_taps, down_weight=down_weight, norm_gain=norm_gain, norm_shift=norm_shift)


def causal_mix(pre, kernel_taps):
    leading = jnp.zeros((2, pre.shape[1]), jnp.float32)
    padded = jnp.concatenate([leading, pre.astype(jnp.float32)], axis=0)
    length = pre.shape[0]
    return kernel_taps[0] * padded[0:length] + kernel_taps[1] * padded[1:length + 1] + kernel_taps[2] * padded[2:length + 2]

def one_sequence(rows, gate_weight, value_weight, gate_taps, value_taps, down_weight, norm_gain, norm_shift):
    gate_pre = jnp.dot(rows, gate_weight, preferred_element_type=jnp.float32).astype(jnp.bfloat16)
    value_pre = jnp.dot(rows, value_weight, preferred_element_type=jnp.float32).astype(jnp.bfloat16)
    gate_mix = causal_mix(gate_pre, gate_taps)
    value_mix = causal_mix(value_pre, value_taps)
    hidden = (jax.nn.gelu(gate_mix, approximate=False) * value_mix).astype(jnp.bfloat16)
    length = rows.shape[0]
    block_cols = FF // N_TP
    hidden_blocks = hidden.reshape(length, N_TP, block_cols).astype(jnp.float32)
    down_blocks = down_weight.reshape(N_TP, block_cols, D).astype(jnp.float32)
    partials = jnp.einsum('lkf,kfd->kld', hidden_blocks, down_blocks).astype(jnp.bfloat16)
    summed = lax.optimization_barrier(jnp.sum(partials.astype(jnp.float32), axis=0))
    average = lax.optimization_barrier(jnp.mean(summed, axis=1, keepdims=True))
    centered = summed - average
    variance = lax.optimization_barrier(jnp.mean(centered * centered, axis=1, keepdims=True))
    normed = centered * lax.rsqrt(variance + 1e-05) * norm_gain + norm_shift
    return normed.astype(jnp.bfloat16)

def reference(tokens, gate_weight, value_weight, gate_taps, value_taps, down_weight, norm_gain, norm_shift):
    length = TOK_DEV * N_TP
    grouped = tokens.reshape(N_FS, length, D)
    result = lax.map(lambda rows: one_sequence(rows, gate_weight, value_weight, gate_taps, value_taps, down_weight, norm_gain, norm_shift), grouped)
    return result.reshape(N_FS * length, D)
```

```python
import functools

import jax
import jax.numpy as jnp
from jax import lax
from jax.experimental import pallas as pl
from jax.experimental.pallas import tpu as pltpu
from jax.sharding import PartitionSpec as P

MESH = pl.DeviceIdType.MESH
HALO = 16
BITS = 4
GV = (0, 1)
DN = (2, 3)


def kernel(
    dims,
    x_ref, g_ref, v_ref, gt_ref, vt_ref, d_ref, gain_ref, shift_ref,
    out_ref,
    tok, gw, vw, dw, taps, pre_g, pre_v, hid, part, rc, zr,
    tok_r, tz_s, tc_s, halo_r, halo_s, hc_s, tap_r, tap_s,
    w_r, wz_s, wx_s, wy_s, wf_s, rc_r, rc_s, zc_r, zc_s,
):
    nz, nx, ny, nc = dims
    rows, width = x_ref.shape
    depth = g_ref.shape[0]
    units = gw.shape[1] // ny
    cols = d_ref.shape[1]
    length = nc * rows
    bit = rows // BITS
    top = units // 2
    wide = width // 2
    fs = lax.axis_index("fs")
    tp = lax.axis_index("tp")
    z, x = fs // nx, fs % nx
    y, c = tp // nc, tp % nc

    def at(zz=z, xx=x, yy=y, cc=c):
        return {"fs": zz * nx + xx, "tp": yy * nc + cc}

    z_others = [(z + i) % nz for i in range(1, nz)]
    x_others = [(x + i) % nx for i in range(1, nx)]
    y_others = [(y + i) % ny for i in range(1, ny)]
    c_others = [(c + i) % nc for i in range(1, nc)]

    barrier = pltpu.get_barrier_semaphore()
    partners = (
        [at(zz=i) for i in z_others]
        + [at(xx=i) for i in x_others]
        + [at(yy=i) for i in y_others]
        + [at(cc=i) for i in c_others]
    )
    for partner in partners:
        pl.semaphore_signal(barrier, inc=1, device_id=partner, device_id_type=MESH)
    pl.semaphore_wait(barrier, len(partners))

    def copy(src, dst, send, recv, device):
        return pltpu.make_async_remote_copy(
            src_ref=src, dst_ref=dst, send_sem=send, recv_sem=recv,
            device_id=device, device_id_type=MESH,
        )

    def ds(start, size, unit):
        return pl.ds(pl.multiple_of(start, unit), size)

    half = (2 * z) // nz
    near = z + half * (nz - 1 - 2 * z)

    def order(j):
        past = (j - near - 1 + nz) // nz
        f = past * j + (1 - past) * (near - j)
        return f + half * (nz - 1 - 2 * f)

    def inside(zz):
        return (zz >= 0) & (zz < nz)

    def both(step, act):
        for way in range(2):
            zz = z - step + 2 * step * way

            @pl.when(inside(zz))
            def _():
                act(zz, way)

    def piece(kind, zz):
        if kind >= 2:
            return d_ref.at[ds(zz * units + (kind - 2) * top, top, 16)]
        ref = g_ref if kind == 0 else v_ref
        return ref.at[:, ds(zz * units, units, 128)]

    def place(kind, src, yy):
        if kind >= 2:
            return dw.at[ds(yy * units + (kind - 2) * top, top, 16), ds(src * cols, cols, cols)]
        ref = gw if kind == 0 else vw
        return ref.at[ds(src * depth, depth, depth), ds(yy * units, units, 128)]

    def w_z(kind, zz):
        return copy(piece(kind, zz), place(kind, fs, y), wz_s.at[kind, zz], w_r.at[kind, fs, y], at(zz=zz))

    def w_x(kind, src, zz, xx):
        s = zz * nx + x
        return copy(src, place(kind, s, y), wx_s.at[kind, zz, xx], w_r.at[kind, s, y], at(xx=xx))

    def w_y(kind, src, zz, yy):
        s = zz * nx + x
        return copy(src, place(kind, s, y), wy_s.at[kind, zz, yy], w_r.at[kind, s, y], at(yy=yy))

    def w_f(kind, zz, xx, yy):
        if kind % 2 == 0:
            s = zz * nx + xx
            return copy(place(kind, s, y), place(kind, s, y), wf_s.at[kind, zz, xx, yy], w_r.at[kind, s, y], at(yy=yy))
        s = zz * nx + x
        return copy(place(kind, s, yy), place(kind, s, yy), wf_s.at[kind, zz, xx, yy], w_r.at[kind, s, yy], at(xx=xx))

    def w_wait(kind, zz, xx, yy):
        s = zz * nx + xx
        copy(place(kind, s, yy), place(kind, s, yy), wz_s.at[kind, 0], w_r.at[kind, s, yy], partners[0]).wait_recv()

    def spread(kind, src, zz):
        for xx in x_others:
            w_x(kind, src, zz, xx).start()
        for yy in y_others:
            w_y(kind, src, zz, yy).start()

    def own(kinds):
        for kind in kinds:
            spread(kind, piece(kind, z), z)

    def arrive(kinds, zz):
        for kind in kinds:
            w_wait(kind, zz, x, y)
            spread(kind, place(kind, zz * nx + x, y), zz)

    def turn(kinds, zz):
        for kind in kinds:
            if kind % 2 == 0:
                for xx in x_others:
                    w_wait(kind, zz, xx, y)
                    for yy in y_others:
                        w_f(kind, zz, xx, yy).start()
            else:
                for yy in y_others:
                    w_wait(kind, zz, x, yy)
                    for xx in x_others:
                        w_f(kind, zz, xx, yy).start()

    def rest(kinds, zz):
        for kind in kinds:
            if kind % 2 == 0:
                for yy in y_others:
                    w_wait(kind, zz, x, yy)
            else:
                for xx in x_others:
                    w_wait(kind, zz, xx, y)
            for xx in x_others:
                for yy in y_others:
                    w_wait(kind, zz, xx, yy)

    def slot(zz, cc):
        return tok.at[zz, ds(HALO + cc * rows, rows, 16)]

    def chunk(zz, cc, b):
        return tok.at[zz, ds(HALO + cc * rows + b * bit, bit, 16)]

    def tok_z(src, zz, way, b):
        return copy(src, chunk(zz, c, b), tz_s.at[way, zz, b], tok_r.at[zz, c, b], at(zz=z + 1 - 2 * way))

    def tok_c(src, zz, cc):
        return copy(src, slot(zz, c), tc_s.at[zz, cc], tok_r.at[zz, c, 0], at(cc=cc))

    def halo_y(src, zz):
        return copy(src, tok.at[zz, pl.ds(0, HALO)], halo_s.at[zz], halo_r.at[zz], at(yy=y + 1))

    def halo_c(zz, cc):
        lead = tok.at[zz, pl.ds(0, HALO)]
        return copy(lead, lead, hc_s.at[zz, cc], halo_r.at[zz], at(cc=cc))

    def cross(src, tail, zz):
        for cc in c_others:
            tok_c(src, zz, cc).start()

        @pl.when((c == nc - 1) & (y < ny - 1))
        def _():
            halo_y(tail, zz).start()

    def tail(zz):
        return tok.at[zz, ds(HALO + (c + 1) * rows - HALO, HALO, 16)]

    def relay(step, bits):
        def act(zz, way):
            ahead = z + 1 - 2 * way
            for b in bits:
                copy(chunk(zz, c, b), chunk(zz, c, b), tz_s.at[0, 0, 0], tok_r.at[zz, c, b], partners[0]).wait_recv()
                if step < nz - 1:

                    @pl.when(inside(ahead))
                    def _():
                        tok_z(chunk(zz, c, b), zz, way, b).start()

            if bits[-1] == BITS - 1:
                cross(slot(zz, c), tail(zz), zz)

        if step < nz:
            both(step, act)

    def gathered(zz):
        for cc in c_others:
            copy(slot(zz, cc), slot(zz, cc), tz_s.at[0, 0, 0], tok_r.at[zz, cc, 0], partners[0]).wait_recv()

        @pl.when(y > 0)
        def _():
            lead = tok.at[zz, pl.ds(0, HALO)]
            copy(lead, lead, halo_s.at[zz], halo_r.at[zz], partners[0]).wait_recv()

            @pl.when(c == nc - 1)
            def _():
                for cc in c_others:
                    halo_c(zz, cc).start()

    def tap(kind, yy):
        ref = gt_ref if kind == 0 else vt_ref
        return copy(
            ref.at[:, ds(z * units, units, 128)], taps.at[kind, :, ds(y * units, units, 128)],
            tap_s.at[kind, yy], tap_r.at[kind, y], at(yy=yy),
        )

    def tap_wait(kind, yy):
        dst = taps.at[kind, :, ds(yy * units, units, 128)]
        copy(dst, dst, tap_s.at[kind, yy], tap_r.at[kind, yy], partners[0]).wait_recv()

    for step in range(1, nz):
        both(step, lambda zz, way: [w_z(kind, zz).start() for kind in GV])
    own(GV)
    for kind in range(2):
        for yy in y_others:
            tap(kind, yy).start()
    cross(x_ref, x_ref.at[pl.ds(rows - HALO, HALO)], z)

    def middle(way):
        return z + way * (nz - 1 - 2 * z) == nz // 2 - 1

    def down_near(late):
        for way in range(2):
            dest = z + 1 - 2 * way
            wanted = middle(way) if late else jnp.logical_not(middle(way))

            @pl.when(inside(dest) & wanted)
            def _():
                for kind in DN:
                    w_z(kind, dest).start()

    for way in range(2):

        @pl.when(inside(z + 1 - 2 * way))
        def _():
            for b in range(BITS):
                tok_z(x_ref.at[pl.ds(b * bit, bit)], z, way, b).start()

    down_near(False)

    @pl.when(y == 0)
    def _():
        tok[:, 0:HALO, :] = jnp.zeros((nz, HALO, width), jnp.bfloat16)

    tok[z, ds(HALO + c * rows, rows, 16)] = x_ref[...]
    mine = ds(fs * depth, depth, depth)
    here = ds(y * units, units, 128)
    part_units = ds(z * units, units, 128)
    gw[mine, here] = g_ref[:, part_units]
    vw[mine, here] = v_ref[:, part_units]
    dw[here, ds(fs * cols, cols, cols)] = d_ref[part_units, :]
    taps[0, :, here] = gt_ref[:, part_units]
    taps[1, :, here] = vt_ref[:, part_units]

    for k in range(1, nz):
        arrive(GV, order(k))
        turn(GV, order(k - 1))
    relay(1, range(BITS))
    down_near(True)
    turn(GV, order(nz - 1))
    own(DN)
    side = nz // 2
    for k in range(1, side):
        arrive(DN, order(k))
    relay(2, range(BITS // 2))
    for kind in range(2):
        for yy in y_others:
            tap_wait(kind, yy)
    for k in range(nz):
        rest(GV, order(k))

    def f32(ref):
        return ref[...].astype(jnp.float32)

    def mix(pre, w, kind, zz):
        raw = jnp.dot(tok[zz], w[...], preferred_element_type=jnp.float32)
        pre[...] = raw.astype(jnp.bfloat16).astype(jnp.float32)
        return (
            taps[kind, 0:1, :] * pre[pl.ds(HALO - 2, length), :]
            + taps[kind, 1:2, :] * pre[pl.ds(HALO - 1, length), :]
            + taps[kind, 2:3, :] * pre[pl.ds(HALO, length), :]
        )

    def hidden(zz):
        gathered(zz)
        gate = mix(pre_g, gw, 0, zz)
        value = mix(pre_v, vw, 1, zz)
        act = 0.5 * gate * (1.0 + lax.erf(gate * (0.5**0.5)))
        hid[zz] = (act * value).astype(jnp.bfloat16)

    def wing(h):
        return ds(h * wide, wide, wide)

    def block(zz, cc, h):
        return part.at[zz, ds(cc * rows, rows, rows), wing(h)]

    def rc_copy(zz, cc, h):
        return copy(block(zz, cc, h), rc.at[zz, :, wing(h)], rc_s.at[zz, cc, h], rc_r.at[zz, h], at(cc=cc))

    def zc_copy(way, zz, h):
        return copy(block(zz, c, h), zr.at[way, zz, :, wing(h)], zc_s.at[way, zz, h], zc_r.at[way, zz, h], at(zz=z + 1 - 2 * way))

    def zc_wait(way, zz, h):
        dst = zr.at[way, zz, :, wing(h)]
        copy(dst, dst, zc_s.at[way, zz, h], zc_r.at[way, zz, h], partners[0]).wait_recv()

    def product(zz, h):
        part[zz, :, wing(h)] = jnp.dot(
            hid[zz], dw[:, wing(h)], preferred_element_type=jnp.float32
        ).astype(jnp.bfloat16)
        for cc in c_others:
            rc_copy(zz, cc, h).start()

    def pair(zz, h, first):
        for _ in c_others:
            rc_copy(zz, c, h).wait_recv()
            sent = block(zz, c, h)
            sent[...] = (f32(sent) + f32(rc.at[zz, :, wing(h)])).astype(jnp.bfloat16)
        if first:

            @pl.when((z == 0) | (z == nz - 1))
            def _():
                zc_copy(half, zz, h).start()

    def pass_on(pos, j, e):
        way = jnp.where(z == pos, 0, 1)
        dest = z + j * (1 - 2 * way)
        h = e + way * (1 - 2 * e)

        @pl.when((z == pos) | (z == nz - 1 - pos))
        def _():
            zc_wait(way, dest, h)
            sent = block(dest, c, h)
            sent[...] = (f32(sent) + f32(zr.at[way, dest, :, wing(h)])).astype(jnp.bfloat16)
            zc_copy(way, dest, h).start()

    def down_far():
        for step in range(2, nz):
            both(step, lambda zz, way: [w_z(kind, zz).start() for kind in DN])

    def down_ready(ks):
        for k in ks:
            rest(DN, order(k))

    hidden(order(0))
    down_far()
    turn(DN, order(0))
    relay(2, range(BITS // 2, BITS))
    hidden(order(1))
    for k in range(1, side):
        turn(DN, order(k))
    down_ready(range(side))
    product(order(1), half)
    for k in range(2, nz):
        if k > 2:
            relay(k, range(BITS))
        hidden(order(k))
        pair(order(k - 1), half, True)
        product(order(k), half)
    product(order(0), half)
    pair(order(nz - 1), half, True)
    pair(order(0), half, False)

    for k in range(side, nz):
        arrive(DN, order(k))
        turn(DN, order(k))
    for pos in range(1, nz // 2):
        pass_on(pos, 1, 0)
    down_ready(range(side, nz))
    other = 1 - half
    for k in range(nz):
        product(order(nz - 1 - k), other)
        if k > 0:
            pair(order(nz - k), other, True)
    pair(order(0), other, False)
    for pos in range(1, nz // 2):
        for j in range(2, nz - pos):
            pass_on(pos, j, 0)
        for j in range(nz - pos - 1, 1, -1):
            pass_on(pos, j, 1)
    for pos in range(nz // 2, nz - 1):
        for j in range(1, nz - pos):
            pass_on(pos, j, 0)
    for pos in range(1, nz // 2):
        pass_on(pos, 1, 1)
    for pos in range(nz // 2, nz - 1):
        for j in range(nz - pos - 1, 0, -1):
            pass_on(pos, j, 1)

    for way in range(2):
        back = z - 1 + 2 * way

        @pl.when(inside(back))
        def _():
            for h in range(2):
                zc_wait(way, z, h)

        @pl.when(jnp.logical_not(inside(back)))
        def _():
            zr[way, z] = jnp.zeros((rows, width), jnp.bfloat16)

    summed = f32(part.at[z, ds(c * rows, rows, rows)]) + f32(zr.at[0, z]) + f32(zr.at[1, z])
    average = jnp.mean(summed, axis=1, keepdims=True)
    centered = summed - average
    variance = jnp.mean(centered * centered, axis=1, keepdims=True)
    normed = centered * lax.rsqrt(variance + 1e-05) * gain_ref[...] + shift_ref[...]
    out_ref[...] = normed.astype(out_ref.dtype)

    for way in range(2):

        @pl.when(inside(z + 1 - 2 * way))
        def _():
            for step in range(nz - 1):
                zz = z - step + 2 * step * way

                @pl.when(inside(zz))
                def _():
                    for b in range(BITS):
                        tok_z(chunk(zz, c, b), zz, way, b).wait_send()

                dest = z + (step + 1) * (1 - 2 * way)

                @pl.when(inside(dest))
                def _():
                    for h in range(2):
                        zc_copy(way, dest, h).wait_send()

    for zz in range(nz):
        for cc in c_others:
            tok_c(slot(zz, c), zz, cc).wait_send()
            for h in range(2):
                rc_copy(zz, cc, h).wait_send()

        @pl.when((c == nc - 1) & (y < ny - 1))
        def _():
            halo_y(tail(zz), zz).wait_send()

        @pl.when((c == nc - 1) & (y > 0))
        def _():
            for cc in c_others:
                halo_c(zz, cc).wait_send()

    for kind in range(2):
        for yy in y_others:
            tap(kind, yy).wait_send()
    for kind in GV + DN:
        for zz in z_others:
            w_z(kind, zz).wait_send()
        for zz in range(nz):
            src = place(kind, zz * nx + x, y)
            for xx in x_others:
                w_x(kind, src, zz, xx).wait_send()
            for yy in y_others:
                w_y(kind, src, zz, yy).wait_send()
            for xx in x_others:
                for yy in y_others:
                    w_f(kind, zz, xx, yy).wait_send()


def solution(mesh):
    n_fs, n_tp = mesh.shape["fs"], mesh.shape["tp"]
    nc = 2 if n_tp % 2 == 0 else 1
    ny = n_tp // nc

    def local(tokens, gate_weight, value_weight, gate_taps, value_taps, down_weight, gain, shift):
        rows, width = tokens.shape
        depth, held = gate_weight.shape
        count = gate_taps.shape[0]
        nz = 4
        while nz > 2 and (n_fs % nz or held % (128 * nz)):
            nz //= 2
        nx = n_fs // nz
        units = held // nz
        length = nc * rows
        bf16 = jnp.bfloat16
        dma = pltpu.SemaphoreType.DMA
        return pl.pallas_call(
            functools.partial(kernel, (nz, nx, ny, nc)),
            out_shape=jax.ShapeDtypeStruct((rows, width), bf16),
            in_specs=[pl.BlockSpec(memory_space=pltpu.VMEM)] * 8,
            out_specs=pl.BlockSpec(memory_space=pltpu.VMEM),
            scratch_shapes=[
                pltpu.VMEM((nz, HALO + length, width), bf16),
                pltpu.VMEM((width, ny * units), bf16),
                pltpu.VMEM((width, ny * units), bf16),
                pltpu.VMEM((ny * units, width), bf16),
                pltpu.VMEM((2, count, ny * units), jnp.float32),
                pltpu.VMEM((HALO + length, ny * units), jnp.float32),
                pltpu.VMEM((HALO + length, ny * units), jnp.float32),
                pltpu.VMEM((nz, length, ny * units), bf16),
                pltpu.VMEM((nz, length, width), bf16),
                pltpu.VMEM((nz, rows, width), bf16),
                pltpu.VMEM((2, nz, rows, width), bf16),
                dma((nz, nc, BITS)),
                dma((2, nz, BITS)),
                dma((nz, nc)),
                dma((nz,)),
                dma((nz,)),
                dma((nz, nc)),
                dma((2, ny)),
                dma((2, ny)),
                dma((4, n_fs, ny)),
                dma((4, nz)),
                dma((4, nz, nx)),
                dma((4, nz, ny)),
                dma((4, nz, nx, ny)),
                dma((nz, 2)),
                dma((nz, nc, 2)),
                dma((2, nz, 2)),
                dma((2, nz, 2)),
            ],
            compiler_params=pltpu.CompilerParams(
                collective_id=0, has_side_effects=True, vmem_limit_bytes=60 * 2**20
            ),
        )(
            tokens, gate_weight, value_weight, gate_taps, value_taps, down_weight,
            gain.reshape(1, width), shift.reshape(1, width),
        )

    in_specs = (
        P(("fs", "tp"), None),
        P("fs", "tp"),
        P("fs", "tp"),
        P(None, "tp"),
        P(None, "tp"),
        P("tp", "fs"),
        P(),
        P(),
    )
    out_specs = P(("fs", "tp"), None)
    return jax.shard_map(local, mesh=mesh, in_specs=in_specs, out_specs=out_specs, check_vma=False)
```

```python
import functools

import jax
import jax.numpy as jnp
from jax import lax
from jax.experimental import pallas as pl
from jax.experimental.pallas import tpu as pltpu
from jax.sharding import PartitionSpec as P

MESH = pl.DeviceIdType.MESH
HALO = 16
BITS = 4
GV = (0, 1)
DN = (2, 3)


def kernel(
    dims,
    x_ref, g_ref, v_ref, gt_ref, vt_ref, d_ref, gain_ref, shift_ref,
    out_ref,
    tok, gw, vw, dw, taps, pre_g, pre_v, hid, part, rc, zr,
    tok_r, tz_s, tc_s, halo_r, halo_s, hz_s, hc_s, tap_r, tap_s,
    w_r, wz_s, wx_s, wy_s, wf_s, rc_r, rc_s, zc_r, zc_s,
):
    nz, nx, ny, nc = dims
    rows, width = x_ref.shape
    depth = g_ref.shape[0]
    units = gw.shape[1] // ny
    cols = d_ref.shape[1]
    length = nc * rows
    bit = rows // BITS
    top = units // 2
    wide = nx * cols
    fs = lax.axis_index("fs")
    tp = lax.axis_index("tp")
    z, x = fs // nx, fs % nx
    y, c = tp // nc, tp % nc

    def at(zz=z, xx=x, yy=y, cc=c):
        return {"fs": zz * nx + xx, "tp": yy * nc + cc}

    z_others = [(z + i) % nz for i in range(1, nz)]
    x_others = [(x + i) % nx for i in range(1, nx)]
    y_others = [(y + i) % ny for i in range(1, ny)]
    c_others = [(c + i) % nc for i in range(1, nc)]

    barrier = pltpu.get_barrier_semaphore()
    partners = (
        [at(zz=i) for i in z_others]
        + [at(xx=i) for i in x_others]
        + [at(yy=i) for i in y_others]
        + [at(cc=i) for i in c_others]
    )
    for partner in partners:
        pl.semaphore_signal(barrier, inc=1, device_id=partner, device_id_type=MESH)
    pl.semaphore_wait(barrier, len(partners))

    def copy(src, dst, send, recv, device):
        return pltpu.make_async_remote_copy(
            src_ref=src, dst_ref=dst, send_sem=send, recv_sem=recv,
            device_id=device, device_id_type=MESH,
        )

    def ds(start, size, unit):
        return pl.ds(pl.multiple_of(start, unit), size)

    half = (2 * z) // nz
    near = z + half * (nz - 1 - 2 * z)

    def order(j):
        past = (j - near - 1 + nz) // nz
        f = past * j + (1 - past) * (near - j)
        return f + half * (nz - 1 - 2 * f)

    ends = (z == 0) | (z == nz - 1)

    def early(k):
        return jnp.where(ends, order(3 - k), order(k)) if nz > 2 and k in (1, 2) else order(k)

    def late(k):
        return order(5 - k) if nz > 2 and k in (2, 3) else order(k)

    def inside(zz):
        return (zz >= 0) & (zz < nz)

    def inner(act):
        @pl.when(jnp.logical_not(ends))
        def _():
            act()

    def outer(act):
        @pl.when(ends)
        def _():
            act()

    def both(step, act):
        for way in range(2):
            zz = z - step + 2 * step * way

            @pl.when(inside(zz))
            def _():
                act(zz, way)

    def piece(kind, zz):
        if kind >= 2:
            return d_ref.at[ds(zz * units + (kind - 2) * top, top, 16)]
        ref = g_ref if kind == 0 else v_ref
        return ref.at[:, ds(zz * units, units, 128)]

    def place(kind, src, yy):
        if kind >= 2:
            return dw.at[ds(yy * units + (kind - 2) * top, top, 16), ds(src * cols, cols, cols)]
        ref = gw if kind == 0 else vw
        return ref.at[ds(src * depth, depth, depth), ds(yy * units, units, 128)]

    def w_z(kind, zz):
        return copy(piece(kind, zz), place(kind, fs, y), wz_s.at[kind, zz], w_r.at[kind, fs, y], at(zz=zz))

    def w_x(kind, src, zz, xx):
        s = zz * nx + x
        return copy(src, place(kind, s, y), wx_s.at[kind, zz, xx], w_r.at[kind, s, y], at(xx=xx))

    def w_y(kind, src, zz, yy):
        s = zz * nx + x
        return copy(src, place(kind, s, y), wy_s.at[kind, zz, yy], w_r.at[kind, s, y], at(yy=yy))

    def w_f(kind, zz, xx, yy):
        if kind % 2 == 0:
            s = zz * nx + xx
            return copy(place(kind, s, y), place(kind, s, y), wf_s.at[kind, zz, xx, yy], w_r.at[kind, s, y], at(yy=yy))
        s = zz * nx + x
        return copy(place(kind, s, yy), place(kind, s, yy), wf_s.at[kind, zz, xx, yy], w_r.at[kind, s, yy], at(xx=xx))

    def w_wait(kind, zz, xx, yy):
        s = zz * nx + xx
        copy(place(kind, s, yy), place(kind, s, yy), wz_s.at[kind, 0], w_r.at[kind, s, yy], partners[0]).wait_recv()

    def spread(kind, src, zz):
        for xx in x_others:
            w_x(kind, src, zz, xx).start()
        for yy in y_others:
            w_y(kind, src, zz, yy).start()

    def own(kinds):
        for kind in kinds:
            spread(kind, piece(kind, z), z)

    def arrive(kinds, zz):
        for kind in kinds:
            w_wait(kind, zz, x, y)
            spread(kind, place(kind, zz * nx + x, y), zz)

    def turn(kinds, zz):
        for kind in kinds:
            if kind % 2 == 0:
                for xx in x_others:
                    w_wait(kind, zz, xx, y)
                    for yy in y_others:
                        w_f(kind, zz, xx, yy).start()
            else:
                for yy in y_others:
                    w_wait(kind, zz, x, yy)
                    for xx in x_others:
                        w_f(kind, zz, xx, yy).start()

    def rest(kinds, zz):
        for kind in kinds:
            if kind % 2 == 0:
                for yy in y_others:
                    w_wait(kind, zz, x, yy)
            else:
                for xx in x_others:
                    w_wait(kind, zz, xx, y)
            for xx in x_others:
                for yy in y_others:
                    w_wait(kind, zz, xx, yy)

    def slot(zz, cc):
        return tok.at[zz, ds(HALO + cc * rows, rows, 16)]

    def chunk(zz, cc, b):
        return tok.at[zz, ds(HALO + cc * rows + b * bit, bit, 16)]

    def tok_z(src, zz, way, b):
        return copy(src, chunk(zz, c, b), tz_s.at[way, zz, b], tok_r.at[zz, c, b], at(zz=z + 1 - 2 * way))

    def tok_c(src, zz, cc):
        return copy(src, slot(zz, c), tc_s.at[zz, cc], tok_r.at[zz, c, 0], at(cc=cc))

    keeper = (c == nc - 1) & (y > 0)

    def lead(zz):
        return tok.at[zz, pl.ds(0, HALO)]

    def halo_y():
        return copy(x_ref.at[pl.ds(rows - HALO, HALO)], lead(z), halo_s.at[z], halo_r.at[z], at(yy=y + 1))

    def halo_z(zz, way):
        return copy(lead(zz), lead(zz), hz_s.at[way, zz], halo_r.at[zz], at(zz=z + 1 - 2 * way))

    def halo_c(zz, cc):
        return copy(lead(zz), lead(zz), hc_s.at[zz, cc], halo_r.at[zz], at(cc=cc))

    def halo_wait(zz):
        copy(lead(zz), lead(zz), hc_s.at[zz, 0], halo_r.at[zz], partners[0]).wait_recv()

    def keep(zz, ways, further):
        @pl.when(keeper)
        def _():
            halo_wait(zz)
            if further:
                for way in ways:

                    @pl.when(inside(z + 1 - 2 * way))
                    def _():
                        halo_z(zz, way).start()

            for cc in c_others:
                halo_c(zz, cc).start()

    def cross(src, zz):
        for cc in c_others:
            tok_c(src, zz, cc).start()

    def relay(step, bits):
        for way in (half, 1 - half):
            zz = z - step + 2 * step * way
            ahead = z + 1 - 2 * way

            @pl.when(inside(zz))
            def _():
                for b in bits:
                    copy(chunk(zz, c, b), chunk(zz, c, b), tz_s.at[0, 0, 0], tok_r.at[zz, c, b], partners[0]).wait_recv()
                    if step < nz - 1:

                        @pl.when(inside(ahead))
                        def _():
                            tok_z(chunk(zz, c, b), zz, way, b).start()

                if bits[-1] == BITS - 1:
                    cross(slot(zz, c), zz)
                    keep(zz, (way,), step < nz - 1)

    def gathered(zz):
        for cc in c_others:
            copy(slot(zz, cc), slot(zz, cc), tz_s.at[0, 0, 0], tok_r.at[zz, cc, 0], partners[0]).wait_recv()

        @pl.when((y > 0) & (c < nc - 1))
        def _():
            halo_wait(zz)

    def tap(kind, yy):
        ref = gt_ref if kind == 0 else vt_ref
        return copy(
            ref.at[:, ds(z * units, units, 128)], taps.at[kind, :, ds(y * units, units, 128)],
            tap_s.at[kind, yy], tap_r.at[kind, y], at(yy=yy),
        )

    def tap_wait(kind, yy):
        dst = taps.at[kind, :, ds(yy * units, units, 128)]
        copy(dst, dst, tap_s.at[kind, yy], tap_r.at[kind, yy], partners[0]).wait_recv()

    def place_of(way):
        return z + way * (nz - 1 - 2 * z)

    def line(kinds, way, steps, wanted=True):
        for step in steps:
            zz = z + step * (1 - 2 * way)

            @pl.when(inside(zz) & wanted)
            def _():
                for kind in kinds:
                    w_z(kind, zz).start()

    central = nz // 2 - 1

    @pl.when((c == nc - 1) & (y < ny - 1))
    def _():
        halo_y().start()

    own(GV)
    for way in range(2):
        pos = place_of(way)
        line(GV, way, (1,), pos == 0)
        line(GV, way, range(nz - 1, 0, -1), pos > 0)

        @pl.when(inside(z + 1 - 2 * way))
        def _():
            for b in range(BITS):
                tok_z(x_ref.at[pl.ds(b * bit, bit)], z, way, b).start()

        line(GV, way, range(nz - 1, 1, -1), pos == 0)
        line(DN, way, (1,), pos != central)
    for kind in range(2):
        for yy in y_others:
            tap(kind, yy).start()
    cross(x_ref, z)

    @pl.when(y == 0)
    def _():
        tok[:, 0:HALO, :] = jnp.zeros((nz, HALO, width), jnp.bfloat16)

    tok[z, ds(HALO + c * rows, rows, 16)] = x_ref[...]
    mine = ds(fs * depth, depth, depth)
    here = ds(y * units, units, 128)
    part_units = ds(z * units, units, 128)
    gw[mine, here] = g_ref[:, part_units]
    vw[mine, here] = v_ref[:, part_units]
    dw[here, ds(fs * cols, cols, cols)] = d_ref[part_units, :]
    taps[0, :, here] = gt_ref[:, part_units]
    taps[1, :, here] = vt_ref[:, part_units]

    keep(z, range(2), True)
    side = nz // 2
    for k in range(1, nz):
        if k == nz - 1:
            turn(GV, early(k - 1))
        arrive(GV, early(k))
        if k < nz - 1:
            turn(GV, early(k - 1))
    relay(1, range(BITS))
    for way in range(2):
        line(DN, way, range(nz - 1, 0, -1), place_of(way) == central)
    turn(GV, order(nz - 1))
    own(DN)
    for way in range(2):
        line(DN, way, range(2, nz), place_of(way) < central)
    if nz > 2:
        arrive(DN[:1], order(1))
        outer(lambda: relay(2, range(BITS)))
    for kind in range(2):
        for yy in y_others:
            tap_wait(kind, yy)
    for k in range(nz):
        rest(GV, order(k))

    def f32(ref):
        return ref[...].astype(jnp.float32)

    def mix(pre, w, kind, zz):
        raw = jnp.dot(tok[zz], w[...], preferred_element_type=jnp.float32)
        pre[...] = raw.astype(jnp.bfloat16).astype(jnp.float32)
        return (
            taps[kind, 0:1, :] * pre[pl.ds(HALO - 2, length), :]
            + taps[kind, 1:2, :] * pre[pl.ds(HALO - 1, length), :]
            + taps[kind, 2:3, :] * pre[pl.ds(HALO, length), :]
        )

    def hidden(zz):
        gathered(zz)
        gate = mix(pre_g, gw, 0, zz)
        value = mix(pre_v, vw, 1, zz)
        act = 0.5 * gate * (1.0 + lax.erf(gate * (0.5**0.5)))
        hid[zz] = (act * value).astype(jnp.bfloat16)

    def wing(h):
        return ds(h * wide, wide, wide)

    def block(zz, cc, h):
        return part.at[zz, ds(cc * rows, rows, rows), wing(h)]

    def rc_copy(zz, cc, h):
        return copy(block(zz, cc, h), rc.at[zz, :, wing(h)], rc_s.at[zz, cc, h], rc_r.at[zz, h], at(cc=cc))

    def zc_copy(way, zz, h):
        return copy(block(zz, c, h), zr.at[way, zz, :, wing(h)], zc_s.at[way, zz, h], zc_r.at[way, zz, h], at(zz=z + 1 - 2 * way))

    def zc_wait(way, zz, h):
        dst = zr.at[way, zz, :, wing(h)]
        copy(dst, dst, zc_s.at[way, zz, h], zc_r.at[way, zz, h], partners[0]).wait_recv()

    def product(zz, h):
        part[zz, :, wing(h)] = jnp.dot(
            hid[zz], dw[:, wing(h)], preferred_element_type=jnp.float32
        ).astype(jnp.bfloat16)
        for cc in c_others:
            rc_copy(zz, cc, h).start()

    def pair(zz, h):
        for _ in c_others:
            rc_copy(zz, c, h).wait_recv()
            sent = block(zz, c, h)
            sent[...] = (f32(sent) + f32(rc.at[zz, :, wing(h)])).astype(jnp.bfloat16)

    def leave(zz, h):
        @pl.when(ends)
        def _():
            zc_copy(half, zz, h).start()

    def pass_on(pos, j, e):
        way = jnp.where(z == pos, 0, 1)
        dest = z + j * (1 - 2 * way)
        e = 5 - e if e > 1 else e
        h = e + way * (nz - 1 - 2 * e)

        @pl.when((z == pos) | (z == nz - 1 - pos))
        def _():
            zc_wait(way, dest, h)
            sent = block(dest, c, h)
            sent[...] = (f32(sent) + f32(zr.at[way, dest, :, wing(h)])).astype(jnp.bfloat16)
            zc_copy(way, dest, h).start()

    def stage(k, turns, now=()):
        h = late(k)
        for i, t in enumerate(turns + [None]):
            if t is not None:
                product(order(t), h)
            if i > 0:
                pair(order(turns[i - 1]), h)
                if turns[i - 1] in now:
                    leave(order(turns[i - 1]), h)

    if nz > 2:
        inner(lambda: relay(2, (0,)))
        hidden(order(2))
        turn(DN, order(0))
        arrive(DN[1:], order(1))
        arrive(DN[:1], late(2))
        inner(lambda: relay(2, (1,)))
        hidden(order(1))
        inner(lambda: relay(2, (2,)))
        rest(DN, order(0))
        stage(0, [2, 1], (2, 1))
        turn(DN, order(1))
        arrive(DN[1:], late(2))
        inner(lambda: relay(2, range(3, BITS)))
        rest(DN, order(1))
        stage(1, [2, 1], (2, 1))
        turn(DN, late(2))
        arrive(DN, late(3))
        relay(3, range(BITS))
        hidden(order(3))
        stage(0, [3], (3,))
        stage(1, [3], (3,))
        pass_on(1, 1, 0)
        pass_on(1, 1, 1)
        rest(DN, late(2))
        stage(2, [3, 2, 1], (3, 2))
        turn(DN, late(3))
        hidden(order(0))
        for k in range(3):
            product(order(0), late(k))
        pass_on(1, 2, 0)
        pass_on(1, 2, 1)
        rest(DN, late(3))
        stage(3, [3, 2, 1], (3, 2))
        leave(order(1), late(2))
        leave(order(1), late(3))
        product(order(0), late(3))
        pass_on(2, 1, 0)
        pass_on(1, 2, 2)
        pass_on(1, 1, 2)
        pass_on(2, 1, 1)
        pass_on(2, 1, 2)
        pass_on(1, 2, 3)
        pass_on(1, 1, 3)
        pass_on(2, 1, 3)
        for k in range(nz):
            pair(order(0), order(k))
    else:
        hidden(order(1))
        hidden(order(0))
        turn(DN, order(0))
        rest(DN, order(0))
        stage(0, [1, 0], (1,))
        arrive(DN, order(1))
        turn(DN, order(1))
        rest(DN, order(1))
        stage(1, [1, 0], (1,))

    for way in range(2):
        back = z - 1 + 2 * way

        @pl.when(inside(back))
        def _():
            for h in range(nz):
                zc_wait(way, z, h)

        @pl.when(jnp.logical_not(inside(back)))
        def _():
            zr[way, z] = jnp.zeros((rows, width), jnp.bfloat16)

    def finish():
        summed = f32(part.at[z, ds(c * rows, rows, rows)]) + f32(zr.at[0, z]) + f32(zr.at[1, z])
        average = jnp.mean(summed, axis=1, keepdims=True)
        centered = summed - average
        variance = jnp.mean(centered * centered, axis=1, keepdims=True)
        normed = centered * lax.rsqrt(variance + 1e-05) * gain_ref[...] + shift_ref[...]
        out_ref[...] = normed.astype(out_ref.dtype)

    finish()

    for way in range(2):

        @pl.when(inside(z + 1 - 2 * way))
        def _():
            for step in range(nz - 1):
                zz = z - step + 2 * step * way

                @pl.when(inside(zz))
                def _():
                    for b in range(BITS):
                        tok_z(chunk(zz, c, b), zz, way, b).wait_send()

                    @pl.when(keeper)
                    def _():
                        halo_z(zz, way).wait_send()

                dest = z + (step + 1) * (1 - 2 * way)

                @pl.when(inside(dest))
                def _():
                    for h in range(nz):
                        zc_copy(way, dest, h).wait_send()

    for zz in range(nz):
        for cc in c_others:
            tok_c(slot(zz, c), zz, cc).wait_send()
            for h in range(nz):
                rc_copy(zz, cc, h).wait_send()

        @pl.when(keeper)
        def _():
            for cc in c_others:
                halo_c(zz, cc).wait_send()

    @pl.when((c == nc - 1) & (y < ny - 1))
    def _():
        halo_y().wait_send()

    for kind in range(2):
        for yy in y_others:
            tap(kind, yy).wait_send()
    for kind in GV + DN:
        for zz in z_others:
            w_z(kind, zz).wait_send()
        for zz in range(nz):
            src = place(kind, zz * nx + x, y)
            for xx in x_others:
                w_x(kind, src, zz, xx).wait_send()
            for yy in y_others:
                w_y(kind, src, zz, yy).wait_send()
            for xx in x_others:
                for yy in y_others:
                    w_f(kind, zz, xx, yy).wait_send()


def solution(mesh):
    n_fs, n_tp = mesh.shape["fs"], mesh.shape["tp"]
    nc = 2 if n_tp % 2 == 0 else 1
    ny = n_tp // nc

    def local(tokens, gate_weight, value_weight, gate_taps, value_taps, down_weight, gain, shift):
        rows, width = tokens.shape
        depth, held = gate_weight.shape
        count = gate_taps.shape[0]
        nz = 4
        while nz > 2 and (n_fs % nz or held % (128 * nz)):
            nz //= 2
        nx = n_fs // nz
        units = held // nz
        length = nc * rows
        bf16 = jnp.bfloat16
        dma = pltpu.SemaphoreType.DMA
        return pl.pallas_call(
            functools.partial(kernel, (nz, nx, ny, nc)),
            out_shape=jax.ShapeDtypeStruct((rows, width), bf16),
            in_specs=[pl.BlockSpec(memory_space=pltpu.VMEM)] * 8,
            out_specs=pl.BlockSpec(memory_space=pltpu.VMEM),
            scratch_shapes=[
                pltpu.VMEM((nz, HALO + length, width), bf16),
                pltpu.VMEM((width, ny * units), bf16),
                pltpu.VMEM((width, ny * units), bf16),
                pltpu.VMEM((ny * units, width), bf16),
                pltpu.VMEM((2, count, ny * units), jnp.float32),
                pltpu.VMEM((HALO + length, ny * units), jnp.float32),
                pltpu.VMEM((HALO + length, ny * units), jnp.float32),
                pltpu.VMEM((nz, length, ny * units), bf16),
                pltpu.VMEM((nz, length, width), bf16),
                pltpu.VMEM((nz, rows, width), bf16),
                pltpu.VMEM((2, nz, rows, width), bf16),
                dma((nz, nc, BITS)),
                dma((2, nz, BITS)),
                dma((nz, nc)),
                dma((nz,)),
                dma((nz,)),
                dma((2, nz)),
                dma((nz, nc)),
                dma((2, ny)),
                dma((2, ny)),
                dma((4, n_fs, ny)),
                dma((4, nz)),
                dma((4, nz, nx)),
                dma((4, nz, ny)),
                dma((4, nz, nx, ny)),
                dma((nz, nz)),
                dma((nz, nc, nz)),
                dma((2, nz, nz)),
                dma((2, nz, nz)),
            ],
            compiler_params=pltpu.CompilerParams(
                collective_id=0, has_side_effects=True, vmem_limit_bytes=60 * 2**20
            ),
        )(
            tokens, gate_weight, value_weight, gate_taps, value_taps, down_weight,
            gain.reshape(1, width), shift.reshape(1, width),
        )

    in_specs = (
        P(("fs", "tp"), None),
        P("fs", "tp"),
        P("fs", "tp"),
        P(None, "tp"),
        P(None, "tp"),
        P("tp", "fs"),
        P(),
        P(),
    )
    out_specs = P(("fs", "tp"), None)
    return jax.shard_map(local, mesh=mesh, in_specs=in_specs, out_specs=out_specs, check_vma=False)
```

```python
import functools

import jax
import jax.numpy as jnp
from jax import lax
from jax.experimental import pallas as pl
from jax.experimental.pallas import tpu as pltpu
from jax.sharding import PartitionSpec as P

MESH = pl.DeviceIdType.MESH
HALO = 16
BITS = 4
GV = (0, 1)
DN = (2, 3)


def kernel(
    dims,
    x_hbm, g_hbm, v_hbm, gt_hbm, vt_hbm, d_hbm, gain_hbm, shift_hbm,
    out_ref,
    g_ref, v_ref, tapin, d_ref, gain_ref, shift_ref, in_s,
    tok, gw, vw, dw, taps, pre_g, pre_v, hid, part, rc, zr,
    tok_r, tokc_r, tz_s, tc_s, halo_r, halo_s, hz_s, hc_s, tap_r, tap_s,
    wl_r, wt_r, wr_r, w_s, rc_r, rc_s, zc_r, zc_s,
):
    nz, nx, ny, nc = dims
    rows, width = x_hbm.shape
    depth = g_ref.shape[0]
    units = gw.shape[1] // ny
    cols = d_ref.shape[1]
    length = nc * rows
    bit = rows // BITS
    top = units // 2
    wide = nx * cols
    fs = lax.axis_index("fs")
    tp = lax.axis_index("tp")
    z, x = fs // nx, fs % nx
    y, c = tp // nc, tp % nc

    def at(zz=z, xx=x, yy=y, cc=c):
        return {"fs": zz * nx + xx, "tp": yy * nc + cc}

    z_others = [(z + i) % nz for i in range(1, nz)]
    x_others = [(x + i) % nx for i in range(1, nx)]
    y_others = [(y + i) % ny for i in range(1, ny)]
    c_others = [(c + i) % nc for i in range(1, nc)]

    def ds(start, size, unit):
        return pl.ds(pl.multiple_of(start, unit), size)

    mine = ds(fs * depth, depth, depth)
    here = ds(y * units, units, 128)
    part_units = ds(z * units, units, 128)
    moves = [
        (g_hbm, g_ref, 0),
        (v_hbm, v_ref, 1),
        (x_hbm, tok.at[z, ds(HALO + c * rows, rows, 16)], 2),
        (d_hbm, d_ref, 3),
        (gt_hbm, tapin.at[0], 4),
        (vt_hbm, tapin.at[1], 4),
        (g_hbm.at[:, part_units], gw.at[mine, here], 5),
        (v_hbm.at[:, part_units], vw.at[mine, here], 5),
        (d_hbm.at[ds(z * units, units, 16)], dw.at[ds(y * units, units, 16), ds(fs * cols, cols, cols)], 5),
        (gt_hbm.at[:, part_units], taps.at[0, :, here], 6),
        (vt_hbm.at[:, part_units], taps.at[1, :, here], 6),
        (gain_hbm, gain_ref, 7),
        (shift_hbm, shift_ref, 8),
    ]
    for src, dst, i in moves:
        pltpu.make_async_copy(src, dst, in_s.at[i]).start()

    def loaded(i):
        whole = [
            g_ref, v_ref, slot_z, d_ref, tapin, gw.at[pl.ds(0, 3 * depth), pl.ds(0, units)],
            taps.at[:, :, here], gain_ref, shift_ref,
        ][i]
        pltpu.make_async_copy(whole, whole, in_s.at[i]).wait()

    slot_z = tok.at[z, ds(HALO + c * rows, rows, 16)]

    barrier = pltpu.get_barrier_semaphore()
    partners = (
        [at(zz=i) for i in z_others]
        + [at(xx=i) for i in x_others]
        + [at(yy=i) for i in y_others]
        + [at(cc=i) for i in c_others]
    )
    for partner in partners:
        pl.semaphore_signal(barrier, inc=1, device_id=partner, device_id_type=MESH)
    pl.semaphore_wait(barrier, len(partners))

    def copy(src, dst, send, recv, device):
        return pltpu.make_async_remote_copy(
            src_ref=src, dst_ref=dst, send_sem=send, recv_sem=recv,
            device_id=device, device_id_type=MESH,
        )

    half = (2 * z) // nz
    near = z + half * (nz - 1 - 2 * z)

    def order(j):
        past = (j - near - 1 + nz) // nz
        f = past * j + (1 - past) * (near - j)
        return f + half * (nz - 1 - 2 * f)

    ends = (z == 0) | (z == nz - 1)

    def early(k):
        return jnp.where(ends, order(3 - k), order(k)) if nz > 2 and k in (1, 2) else order(k)

    def late(k):
        return order(5 - k) if nz > 2 and k in (2, 3) else order(k)

    def inside(zz):
        return (zz >= 0) & (zz < nz)

    def inner(act):
        @pl.when(jnp.logical_not(ends))
        def _():
            act()

    def outer(act):
        @pl.when(ends)
        def _():
            act()

    def piece(kind, zz):
        if kind >= 2:
            return d_ref.at[ds(zz * units + (kind - 2) * top, top, 16)]
        ref = g_ref if kind == 0 else v_ref
        return ref.at[:, ds(zz * units, units, 128)]

    def place(kind, src, yy):
        if kind >= 2:
            return dw.at[ds(yy * units + (kind - 2) * top, top, 16), ds(src * cols, cols, cols)]
        ref = gw if kind == 0 else vw
        return ref.at[ds(src * depth, depth, depth), ds(yy * units, units, 128)]

    def bulk(kind, a, b):
        if kind >= 2:
            return dw.at[pl.ds(0, top * b), pl.ds(0, cols * a)]
        return gw.at[pl.ds(0, depth * a), pl.ds(0, units * b)]

    def final(kind, zz):
        return wr_r.at[kind if kind < 2 else 2 + (kind - 2) * nz + zz]

    def await_recv(ref, sem):
        copy(ref, ref, w_s.at[0, 0], sem, partners[0]).wait_recv()

    def await_send(ref, sem):
        copy(ref, ref, sem, wl_r.at[0, 0], partners[0]).wait_send()

    def w_z(kind, zz):
        return copy(piece(kind, zz), place(kind, fs, y), w_s.at[kind, 0], wl_r.at[kind // 2, z], at(zz=zz))

    def spread(kind, src, zz):
        dst = place(kind, zz * nx + x, y)
        for i, xx in enumerate(x_others):
            recv = wt_r.at[kind, zz, nx - i - 2] if kind % 2 == 0 else final(kind, zz)
            copy(src, dst, w_s.at[kind, 1], recv, at(xx=xx)).start()
        for i, yy in enumerate(y_others):
            recv = wt_r.at[kind, zz, ny - i - 2] if kind % 2 == 1 else final(kind, zz)
            copy(src, dst, w_s.at[kind, 2], recv, at(yy=yy)).start()

    def own(kinds):
        for kind in kinds:
            spread(kind, piece(kind, z), z)

    def arrive(kinds, zz):
        for kind in kinds:
            if kind % 2 == 0:
                await_recv(bulk(kind, 2, 1) if kind < 2 else bulk(kind, 1, 2), wl_r.at[kind // 2, zz])
            spread(kind, place(kind, zz * nx + x, y), zz)

    def turn(kinds, zz):
        for kind in kinds:
            across, along = (x_others, y_others) if kind % 2 == 0 else (y_others, x_others)
            for i, a in enumerate(across):
                ref = place(kind, zz * nx + a, y) if kind % 2 == 0 else place(kind, zz * nx + x, a)
                await_recv(ref, wt_r.at[kind, zz, i])
                for b in along:
                    device = at(yy=b) if kind % 2 == 0 else at(xx=b)
                    copy(ref, ref, w_s.at[kind, 3], final(kind, zz), device).start()

    def rest(kinds, zz):
        for kind in kinds:
            a = nx if kind % 2 == 0 else nx - 1
            b = ny - 1 if kind % 2 == 0 else ny
            if a and b:
                await_recv(bulk(kind, a * nz if kind < 2 else a, b), final(kind, zz))

    def slot(zz, cc):
        return tok.at[zz, ds(HALO + cc * rows, rows, 16)]

    def chunk(zz, cc, b):
        return tok.at[zz, ds(HALO + cc * rows + b * bit, bit, 16)]

    def tok_z(src, zz, way, b):
        return copy(src, chunk(zz, c, b), tz_s.at[way], tok_r.at[zz, b], at(zz=z + 1 - 2 * way))

    def tok_c(src, zz, cc):
        return copy(src, slot(zz, c), tc_s.at[0], tokc_r.at[zz], at(cc=cc))

    keeper = (c == nc - 1) & (y > 0)

    def lead(zz):
        return tok.at[zz, pl.ds(0, HALO)]

    def halo_y():
        return copy(tok.at[z, ds(c * rows + rows, HALO, 16)], lead(z), halo_s.at[0], halo_r.at[z], at(yy=y + 1))

    def halo_z(zz, way):
        return copy(lead(zz), lead(zz), hz_s.at[way], halo_r.at[zz], at(zz=z + 1 - 2 * way))

    def halo_c(zz, cc):
        return copy(lead(zz), lead(zz), hc_s.at[0], halo_r.at[zz], at(cc=cc))

    def halo_wait(zz):
        await_recv(lead(zz), halo_r.at[zz])

    def keep(zz, ways, further):
        @pl.when(keeper)
        def _():
            halo_wait(zz)
            if further:
                for way in ways:

                    @pl.when(inside(z + 1 - 2 * way))
                    def _():
                        halo_z(zz, way).start()

            for cc in c_others:
                halo_c(zz, cc).start()

    def cross(src, zz):
        for cc in c_others:
            tok_c(src, zz, cc).start()

    def relay(step, bits):
        for way in (half, 1 - half):
            zz = z - step + 2 * step * way
            ahead = z + 1 - 2 * way

            @pl.when(inside(zz))
            def _():
                for b in bits:
                    await_recv(chunk(zz, c, b), tok_r.at[zz, b])
                    if step < nz - 1:

                        @pl.when(inside(ahead))
                        def _():
                            tok_z(chunk(zz, c, b), zz, way, b).start()

                if bits[-1] == BITS - 1:
                    cross(slot(zz, c), zz)
                    keep(zz, (way,), step < nz - 1)

    def gathered(zz):
        for cc in c_others:
            await_recv(slot(zz, cc), tokc_r.at[zz])

        @pl.when((y > 0) & (c < nc - 1))
        def _():
            halo_wait(zz)

    def tap(kind, yy):
        return copy(tapin.at[kind, :, part_units], taps.at[kind, :, here], tap_s.at[0], tap_r.at[0], at(yy=yy))

    def tap_bulk():
        return taps.at[:, :, pl.ds(0, units * (ny - 1))]

    def place_of(way):
        return z + way * (nz - 1 - 2 * z)

    def line(kinds, way, steps, wanted=True):
        for step in steps:
            zz = z + step * (1 - 2 * way)

            @pl.when(inside(zz) & wanted)
            def _():
                for kind in kinds:
                    w_z(kind, zz).start()

    central = nz // 2 - 1

    loaded(0)
    loaded(1)
    own(GV)
    for way in range(2):
        pos = place_of(way)
        line(GV, way, (1,), pos == 0)
        line(GV, way, range(nz - 1, 0, -1), pos > 0)
    loaded(2)

    @pl.when((c == nc - 1) & (y < ny - 1))
    def _():
        halo_y().start()

    for way in range(2):
        pos = place_of(way)

        @pl.when(inside(z + 1 - 2 * way))
        def _():
            for b in range(BITS):
                tok_z(chunk(z, c, b), z, way, b).start()

        line(GV, way, range(nz - 1, 1, -1), pos == 0)
    loaded(3)
    loaded(4)
    for way in range(2):
        line(DN, way, (1,), place_of(way) != central)
    for kind in range(2):
        for yy in y_others:
            tap(kind, yy).start()
    cross(slot(z, c), z)

    @pl.when(y == 0)
    def _():
        tok[:, 0:HALO, :] = jnp.zeros((nz, HALO, width), jnp.bfloat16)

    keep(z, range(2), True)
    side = nz // 2
    for k in range(1, nz):
        first = k in (1, nz - 1)
        if first:
            turn(GV, early(k - 1))
        arrive(GV, early(k))
        if not first:
            turn(GV, early(k - 1))
    relay(1, range(BITS))
    for way in range(2):
        line(DN, way, range(nz - 1, 0, -1), place_of(way) == central)
    turn(GV, order(nz - 1))
    own(DN)
    for way in range(2):
        line(DN, way, range(2, nz), place_of(way) < central)
    if nz > 2:
        arrive(DN[:1], order(1))
        outer(lambda: relay(2, range(BITS)))
    for i in range(5, 9):
        loaded(i)
    if ny > 1:
        await_recv(tap_bulk(), tap_r.at[0])
    rest(GV, 0)

    def f32(ref):
        return ref[...].astype(jnp.float32)

    def mix(pre, w, kind, zz):
        raw = jnp.dot(tok[zz], w[...], preferred_element_type=jnp.float32)
        pre[...] = raw.astype(jnp.bfloat16).astype(jnp.float32)
        return (
            taps[kind, 0:1, :] * pre[pl.ds(HALO - 2, length), :]
            + taps[kind, 1:2, :] * pre[pl.ds(HALO - 1, length), :]
            + taps[kind, 2:3, :] * pre[pl.ds(HALO, length), :]
        )

    def hidden(zz):
        gathered(zz)
        gate = mix(pre_g, gw, 0, zz)
        value = mix(pre_v, vw, 1, zz)
        act = 0.5 * gate * (1.0 + lax.erf(gate * (0.5**0.5)))
        hid[zz] = (act * value).astype(jnp.bfloat16)

    def wing(h):
        return ds(h * wide, wide, wide)

    def block(zz, cc, h):
        return part.at[zz, ds(cc * rows, rows, rows), wing(h)]

    def rc_copy(zz, cc, h):
        return copy(block(zz, cc, h), rc.at[zz, :, wing(h)], rc_s.at[0], rc_r.at[zz, h], at(cc=cc))

    def zc_copy(way, zz, h):
        ahead = z + 1 - 2 * way
        recv = zc_r.at[jnp.where(zz == ahead, nz * nz + way, zz * nz + h)]
        return copy(block(zz, c, h), zr.at[way, zz, :, wing(h)], zc_s.at[way], recv, at(zz=ahead))

    def zc_wait(way, zz, h):
        await_recv(zr.at[way, zz, :, wing(h)], zc_r.at[zz * nz + h])

    def product(zz, h):
        part[zz, :, wing(h)] = jnp.dot(
            hid[zz], dw[:, wing(h)], preferred_element_type=jnp.float32
        ).astype(jnp.bfloat16)
        for cc in c_others:
            rc_copy(zz, cc, h).start()

    def pair(zz, h):
        for _ in c_others:
            rc_copy(zz, c, h).wait_recv()
            sent = block(zz, c, h)
            sent[...] = (f32(sent) + f32(rc.at[zz, :, wing(h)])).astype(jnp.bfloat16)

    def leave(zz, h):
        @pl.when(ends)
        def _():
            zc_copy(half, zz, h).start()

    def pass_on(pos, j, e):
        way = jnp.where(z == pos, 0, 1)
        dest = z + j * (1 - 2 * way)
        e = 5 - e if e > 1 else e
        h = e + way * (nz - 1 - 2 * e)

        @pl.when((z == pos) | (z == nz - 1 - pos))
        def _():
            zc_wait(way, dest, h)
            sent = block(dest, c, h)
            sent[...] = (f32(sent) + f32(zr.at[way, dest, :, wing(h)])).astype(jnp.bfloat16)
            zc_copy(way, dest, h).start()

    def stage(k, turns, now=()):
        h = late(k)
        for i, t in enumerate(turns + [None]):
            if t is not None:
                product(order(t), h)
            if i > 0:
                pair(order(turns[i - 1]), h)
                if turns[i - 1] in now:
                    leave(order(turns[i - 1]), h)

    if nz > 2:
        inner(lambda: relay(2, (0,)))
        hidden(order(2))
        turn(DN, order(0))
        arrive(DN[1:], order(1))
        inner(lambda: relay(2, (1,)))
        hidden(order(1))
        inner(lambda: relay(2, (2,)))
        rest(DN, order(0))
        stage(0, [2, 1], (2, 1))
        turn(DN, order(1))
        arrive(DN, late(2))
        inner(lambda: relay(2, range(3, BITS)))
        rest(DN, order(1))
        stage(1, [2, 1], (2, 1))
        turn(DN, late(2))
        arrive(DN, late(3))
        relay(3, range(BITS))
        hidden(order(3))
        stage(0, [3], (3,))
        stage(1, [3], (3,))
        pass_on(1, 1, 0)
        pass_on(1, 1, 1)
        rest(DN, late(2))
        stage(2, [3, 2, 1], (3, 2))
        turn(DN, late(3))
        hidden(order(0))
        for k in range(3):
            product(order(0), late(k))
        pass_on(1, 2, 0)
        pass_on(1, 2, 1)
        rest(DN, late(3))
        stage(3, [3, 2, 1], (3, 2))
        leave(order(1), late(2))
        leave(order(1), late(3))
        product(order(0), late(3))
        pass_on(2, 1, 0)
        pass_on(1, 2, 2)
        pass_on(1, 1, 2)
        pass_on(2, 1, 1)
        pass_on(2, 1, 2)
        pass_on(1, 2, 3)
        pass_on(1, 1, 3)
        pass_on(2, 1, 3)
        for k in range(nz):
            pair(order(0), order(k))
    else:
        hidden(order(1))
        hidden(order(0))
        turn(DN, order(0))
        rest(DN, order(0))
        stage(0, [1, 0], (1,))
        arrive(DN, order(1))
        turn(DN, order(1))
        rest(DN, order(1))
        stage(1, [1, 0], (1,))

    for way in range(2):
        for p in range(nz - 1):

            @pl.when(place_of(way) == p)
            def _():
                await_send(part.at[pl.ds(0, p + 1), pl.ds(0, rows)], tz_s.at[way])
                await_send(part.at[pl.ds(0, nz - 1 - p), pl.ds(0, rows)], zc_s.at[way])

                @pl.when(keeper)
                def _():
                    await_send(part.at[pl.ds(0, p + 1), pl.ds(0, HALO)], hz_s.at[way])

    @pl.when((c == nc - 1) & (y < ny - 1))
    def _():
        await_send(lead(z), halo_s.at[0])

    if nc > 1:
        others = part.at[:, pl.ds(0, rows * (nc - 1))]
        await_send(others, tc_s.at[0])
        await_send(others, rc_s.at[0])

        @pl.when(keeper)
        def _():
            await_send(part.at[:, pl.ds(0, HALO * (nc - 1))], hc_s.at[0])

    if ny > 1:
        await_send(tap_bulk(), tap_s.at[0])
    for kind in GV + DN:
        for way, (a, b) in enumerate([(nz - 1, 1), (nz * (nx - 1), 1), (nz, ny - 1), (nz * (nx - 1), ny - 1)]):
            if a and b:
                await_send(bulk(kind, a, b), w_s.at[kind, way])

    for way in range(2):
        back = z - 1 + 2 * way

        @pl.when(inside(back))
        def _():
            await_recv(zr.at[way, z], zc_r.at[nz * nz + way])

        @pl.when(jnp.logical_not(inside(back)))
        def _():
            zr[way, z] = jnp.zeros((rows, width), jnp.bfloat16)

    def finish():
        summed = f32(part.at[z, ds(c * rows, rows, rows)]) + f32(zr.at[0, z]) + f32(zr.at[1, z])
        average = jnp.mean(summed, axis=1, keepdims=True)
        centered = summed - average
        variance = jnp.mean(centered * centered, axis=1, keepdims=True)
        normed = centered * lax.rsqrt(variance + 1e-05) * gain_ref[...] + shift_ref[...]
        out_ref[...] = normed.astype(out_ref.dtype)

    finish()


def solution(mesh):
    n_fs, n_tp = mesh.shape["fs"], mesh.shape["tp"]
    nc = 2 if n_tp % 2 == 0 else 1
    ny = n_tp // nc

    def local(tokens, gate_weight, value_weight, gate_taps, value_taps, down_weight, gain, shift):
        rows, width = tokens.shape
        depth, held = gate_weight.shape
        count = gate_taps.shape[0]
        nz = 4
        while nz > 2 and (n_fs % nz or held % (128 * nz)):
            nz //= 2
        nx = n_fs // nz
        units = held // nz
        length = nc * rows
        bf16 = jnp.bfloat16
        dma = pltpu.SemaphoreType.DMA
        return pl.pallas_call(
            functools.partial(kernel, (nz, nx, ny, nc)),
            out_shape=pltpu.VMEM((rows, width), bf16),
            in_specs=[pl.BlockSpec(memory_space=pltpu.HBM)] * 8,
            out_specs=pl.BlockSpec(memory_space=pltpu.VMEM),
            scratch_shapes=[
                pltpu.VMEM((depth, held), bf16),
                pltpu.VMEM((depth, held), bf16),
                pltpu.VMEM((2, count, held), jnp.float32),
                pltpu.VMEM(down_weight.shape, bf16),
                pltpu.VMEM((1, width), jnp.float32),
                pltpu.VMEM((1, width), jnp.float32),
                dma((9,)),
                pltpu.VMEM((nz, HALO + length, width), bf16),
                pltpu.VMEM((width, ny * units), bf16),
                pltpu.VMEM((width, ny * units), bf16),
                pltpu.VMEM((ny * units, width), bf16),
                pltpu.VMEM((2, count, ny * units), jnp.float32),
                pltpu.VMEM((HALO + length, ny * units), jnp.float32),
                pltpu.VMEM((HALO + length, ny * units), jnp.float32),
                pltpu.VMEM((nz, length, ny * units), bf16),
                pltpu.VMEM((nz, length, width), bf16),
                pltpu.VMEM((nz, rows, width), bf16),
                pltpu.VMEM((2, nz, rows, width), bf16),
                dma((nz, BITS)),
                dma((nz,)),
                dma((2,)),
                dma((1,)),
                dma((nz,)),
                dma((1,)),
                dma((2,)),
                dma((1,)),
                dma((1,)),
                dma((1,)),
                dma((2, nz)),
                dma((4, nz, max(nx, ny, 2) - 1)),
                dma((2 + 2 * nz,)),
                dma((4, 4)),
                dma((nz, nz)),
                dma((1,)),
                dma((nz * nz + 2,)),
                dma((2,)),
            ],
            compiler_params=pltpu.CompilerParams(
                collective_id=0, has_side_effects=True, vmem_limit_bytes=58 * 2**20
            ),
        )(
            tokens, gate_weight, value_weight, gate_taps, value_taps, down_weight,
            gain.reshape(1, width), shift.reshape(1, width),
        )

    in_specs = (
        P(("fs", "tp"), None),
        P("fs", "tp"),
        P("fs", "tp"),
        P(None, "tp"),
        P(None, "tp"),
        P("tp", "fs"),
        P(),
        P(),
    )
    out_specs = P(("fs", "tp"), None)
    return jax.shard_map(local, mesh=mesh, in_specs=in_specs, out_specs=out_specs, check_vma=False)
```

```python
import functools

import jax
import jax.numpy as jnp
from jax import lax
from jax.experimental import pallas as pl
from jax.experimental.pallas import tpu as pltpu
from jax.sharding import PartitionSpec as P

MESH = pl.DeviceIdType.MESH
HALO = 16
BITS = 4
GV = (0, 1)
DN = (2, 3)


def kernel(
    dims,
    x_hbm, g_hbm, v_hbm, gt_hbm, vt_hbm, d_hbm, gain_hbm, shift_hbm,
    out_ref,
    g_ref, v_ref, tapin, d_ref, gain_ref, shift_ref, in_s,
    tok, gw, vw, dw, taps, pre_g, pre_v, hid, part, rc, zr, zx,
    tok_r, tokc_r, tz_s, tc_s, halo_r, halo_s, hz_s, hc_s, tap_r, tap_s,
    wl_r, wt_r, wr_r, w_s, rc_r, rc_s, zc_r, zc_s,
):
    nz, nx, ny, nc = dims
    rows, width = x_hbm.shape
    depth = g_ref.shape[0]
    units = gw.shape[1] // ny
    cols = d_ref.shape[1]
    length = nc * rows
    bit = rows // BITS
    top = units // 2
    wide = nx * cols
    fs = lax.axis_index("fs")
    tp = lax.axis_index("tp")
    z, x = fs // nx, fs % nx
    y, c = tp // nc, tp % nc

    def at(zz=z, xx=x, yy=y, cc=c):
        return {"fs": zz * nx + xx, "tp": yy * nc + cc}

    z_others = [(z + i) % nz for i in range(1, nz)]
    x_others = [(x + i) % nx for i in range(1, nx)]
    y_others = [(y + i) % ny for i in range(1, ny)]
    c_others = [(c + i) % nc for i in range(1, nc)]

    def ds(start, size, unit):
        return pl.ds(pl.multiple_of(start, unit), size)

    mine = ds(fs * depth, depth, depth)
    here = ds(y * units, units, 128)
    part_units = ds(z * units, units, 128)
    moves = [
        (g_hbm, g_ref, 0),
        (v_hbm, v_ref, 1),
        (x_hbm, tok.at[z, ds(HALO + c * rows, rows, 16)], 2),
        (d_hbm, d_ref, 3),
        (gt_hbm, tapin.at[0], 4),
        (vt_hbm, tapin.at[1], 4),
        (g_hbm.at[:, part_units], gw.at[mine, here], 5),
        (v_hbm.at[:, part_units], vw.at[mine, here], 5),
        (d_hbm.at[ds(z * units, units, 16)], dw.at[ds(y * units, units, 16), ds(fs * cols, cols, cols)], 5),
        (gt_hbm.at[:, part_units], taps.at[0, :, here], 6),
        (vt_hbm.at[:, part_units], taps.at[1, :, here], 6),
        (gain_hbm, gain_ref, 7),
        (shift_hbm, shift_ref, 8),
    ]
    for src, dst, i in moves:
        pltpu.make_async_copy(src, dst, in_s.at[i]).start()

    def loaded(i):
        whole = [
            g_ref, v_ref, slot_z, d_ref, tapin, gw.at[pl.ds(0, 3 * depth), pl.ds(0, units)],
            taps.at[:, :, here], gain_ref, shift_ref,
        ][i]
        pltpu.make_async_copy(whole, whole, in_s.at[i]).wait()

    slot_z = tok.at[z, ds(HALO + c * rows, rows, 16)]

    barrier = pltpu.get_barrier_semaphore()
    partners = (
        [at(zz=i) for i in z_others]
        + [at(xx=i) for i in x_others]
        + [at(yy=i) for i in y_others]
        + [at(cc=i) for i in c_others]
    )
    for partner in partners:
        pl.semaphore_signal(barrier, inc=1, device_id=partner, device_id_type=MESH)
    pl.semaphore_wait(barrier, len(partners))

    def copy(src, dst, send, recv, device):
        return pltpu.make_async_remote_copy(
            src_ref=src, dst_ref=dst, send_sem=send, recv_sem=recv,
            device_id=device, device_id_type=MESH,
        )

    half = (2 * z) // nz
    near = z + half * (nz - 1 - 2 * z)

    def order(j):
        past = (j - near - 1 + nz) // nz
        f = past * j + (1 - past) * (near - j)
        return f + half * (nz - 1 - 2 * f)

    ends = (z == 0) | (z == nz - 1)

    def early(k):
        return jnp.where(ends, order(3 - k), order(k)) if nz > 2 and k in (1, 2) else order(k)

    def late(k):
        return order(5 - k) if nz > 2 and k in (2, 3) else order(k)

    def inside(zz):
        return (zz >= 0) & (zz < nz)

    def inner(act):
        @pl.when(jnp.logical_not(ends))
        def _():
            act()

    def outer(act):
        @pl.when(ends)
        def _():
            act()

    def piece(kind, zz):
        if kind >= 2:
            return d_ref.at[ds(zz * units + (kind - 2) * top, top, 16)]
        ref = g_ref if kind == 0 else v_ref
        return ref.at[:, ds(zz * units, units, 128)]

    def place(kind, src, yy):
        if kind >= 2:
            return dw.at[ds(yy * units + (kind - 2) * top, top, 16), ds(src * cols, cols, cols)]
        ref = gw if kind == 0 else vw
        return ref.at[ds(src * depth, depth, depth), ds(yy * units, units, 128)]

    def bulk(kind, a, b):
        if kind >= 2:
            return dw.at[pl.ds(0, top * b), pl.ds(0, cols * a)]
        return gw.at[pl.ds(0, depth * a), pl.ds(0, units * b)]

    def final(kind, zz):
        return wr_r.at[kind if kind < 2 else 2 + (kind - 2) * nz + zz]

    def await_recv(ref, sem):
        copy(ref, ref, w_s.at[0, 0], sem, partners[0]).wait_recv()

    def await_send(ref, sem):
        copy(ref, ref, sem, wl_r.at[0, 0], partners[0]).wait_send()

    def w_z(kind, zz):
        return copy(piece(kind, zz), place(kind, fs, y), w_s.at[kind, 0], wl_r.at[kind // 2, z], at(zz=zz))

    def spread(kind, src, zz):
        dst = place(kind, zz * nx + x, y)
        for i, xx in enumerate(x_others):
            recv = wt_r.at[kind, zz, nx - i - 2] if kind % 2 == 0 else final(kind, zz)
            copy(src, dst, w_s.at[kind, 1], recv, at(xx=xx)).start()
        for i, yy in enumerate(y_others):
            recv = wt_r.at[kind, zz, ny - i - 2] if kind % 2 == 1 else final(kind, zz)
            copy(src, dst, w_s.at[kind, 2], recv, at(yy=yy)).start()

    def own(kinds):
        for kind in kinds:
            spread(kind, piece(kind, z), z)

    def arrive(kinds, zz):
        for kind in kinds:
            if kind % 2 == 0:
                await_recv(bulk(kind, 2, 1) if kind < 2 else bulk(kind, 1, 2), wl_r.at[kind // 2, zz])
            spread(kind, place(kind, zz * nx + x, y), zz)

    def turn(kinds, zz):
        for kind in kinds:
            across, along = (x_others, y_others) if kind % 2 == 0 else (y_others, x_others)
            for i, a in enumerate(across):
                ref = place(kind, zz * nx + a, y) if kind % 2 == 0 else place(kind, zz * nx + x, a)
                await_recv(ref, wt_r.at[kind, zz, i])
                for b in along:
                    device = at(yy=b) if kind % 2 == 0 else at(xx=b)
                    copy(ref, ref, w_s.at[kind, 3], final(kind, zz), device).start()

    def rest(kinds, zz):
        for kind in kinds:
            a = nx if kind % 2 == 0 else nx - 1
            b = ny - 1 if kind % 2 == 0 else ny
            if a and b:
                await_recv(bulk(kind, a * nz if kind < 2 else a, b), final(kind, zz))

    def slot(zz, cc):
        return tok.at[zz, ds(HALO + cc * rows, rows, 16)]

    def chunk(zz, cc, b):
        return tok.at[zz, ds(HALO + cc * rows + b * bit, bit, 16)]

    def tok_z(src, zz, way, b):
        return copy(src, chunk(zz, c, b), tz_s.at[way], tok_r.at[zz, b], at(zz=z + 1 - 2 * way))

    def tok_c(src, zz, cc):
        return copy(src, slot(zz, c), tc_s.at[0], tokc_r.at[zz], at(cc=cc))

    keeper = (c == nc - 1) & (y > 0)

    def lead(zz):
        return tok.at[zz, pl.ds(0, HALO)]

    def halo_y():
        return copy(tok.at[z, ds(c * rows + rows, HALO, 16)], lead(z), halo_s.at[0], halo_r.at[z], at(yy=y + 1))

    def halo_z(zz, way):
        return copy(lead(zz), lead(zz), hz_s.at[way], halo_r.at[zz], at(zz=z + 1 - 2 * way))

    def halo_c(zz, cc):
        return copy(lead(zz), lead(zz), hc_s.at[0], halo_r.at[zz], at(cc=cc))

    def halo_wait(zz):
        await_recv(lead(zz), halo_r.at[zz])

    def keep(zz, ways, further):
        @pl.when(keeper)
        def _():
            halo_wait(zz)
            if further:
                for way in ways:

                    @pl.when(inside(z + 1 - 2 * way))
                    def _():
                        halo_z(zz, way).start()

            for cc in c_others:
                halo_c(zz, cc).start()

    def cross(src, zz):
        for cc in c_others:
            tok_c(src, zz, cc).start()

    def relay(step, bits):
        for way in (half, 1 - half):
            zz = z - step + 2 * step * way
            ahead = z + 1 - 2 * way

            @pl.when(inside(zz))
            def _():
                for b in bits:
                    await_recv(chunk(zz, c, b), tok_r.at[zz, b])
                    if step < nz - 1:

                        @pl.when(inside(ahead))
                        def _():
                            tok_z(chunk(zz, c, b), zz, way, b).start()

                if bits[-1] == BITS - 1:
                    cross(slot(zz, c), zz)
                    keep(zz, (way,), step < nz - 1)

    def gathered(zz):
        for cc in c_others:
            await_recv(slot(zz, cc), tokc_r.at[zz])

        @pl.when((y > 0) & (c < nc - 1))
        def _():
            halo_wait(zz)

    def tap(kind, yy):
        return copy(tapin.at[kind, :, part_units], taps.at[kind, :, here], tap_s.at[0], tap_r.at[0], at(yy=yy))

    def tap_bulk():
        return taps.at[:, :, pl.ds(0, units * (ny - 1))]

    def place_of(way):
        return z + way * (nz - 1 - 2 * z)

    def line(kinds, way, steps, wanted=True):
        for step in steps:
            zz = z + step * (1 - 2 * way)

            @pl.when(inside(zz) & wanted)
            def _():
                for kind in kinds:
                    w_z(kind, zz).start()

    central = nz // 2 - 1

    loaded(0)
    loaded(1)
    own(GV)
    for way in range(2):
        pos = place_of(way)
        line(GV, way, (1,), pos == 0)
        line(GV, way, range(nz - 1, 0, -1), pos > 0)
    loaded(2)

    @pl.when((c == nc - 1) & (y < ny - 1))
    def _():
        halo_y().start()

    for way in range(2):
        pos = place_of(way)

        @pl.when(inside(z + 1 - 2 * way))
        def _():
            for b in range(BITS):
                tok_z(chunk(z, c, b), z, way, b).start()

        line(GV, way, range(nz - 1, 1, -1), pos == 0)
    loaded(3)
    loaded(4)
    for way in range(2):
        line(DN, way, (1,), place_of(way) != central)
    for kind in range(2):
        for yy in y_others:
            tap(kind, yy).start()
    cross(slot(z, c), z)

    @pl.when(y == 0)
    def _():
        tok[:, 0:HALO, :] = jnp.zeros((nz, HALO, width), jnp.bfloat16)

    keep(z, range(2), True)
    side = nz // 2
    for k in range(1, nz):
        first = k in (1, nz - 1)
        if first:
            turn(GV, early(k - 1))
        arrive(GV, early(k))
        if not first:
            turn(GV, early(k - 1))
    relay(1, range(BITS))
    for way in range(2):
        line(DN, way, range(1, nz), place_of(way) == central)
    turn(GV, order(nz - 1))
    own(DN)
    for way in range(2):
        line(DN, way, range(2, nz), place_of(way) < central)
    if nz > 2:
        arrive(DN[:1], order(1))
        outer(lambda: relay(2, range(BITS)))
    for i in range(5, 9):
        loaded(i)
    if ny > 1:
        await_recv(tap_bulk(), tap_r.at[0])
    rest(GV, 0)

    def f32(ref):
        return ref[...].astype(jnp.float32)

    def mix(pre, w, kind, zz):
        raw = jnp.dot(tok[zz], w[...], preferred_element_type=jnp.float32)
        pre[...] = raw.astype(jnp.bfloat16).astype(jnp.float32)
        return (
            taps[kind, 0:1, :] * pre[pl.ds(HALO - 2, length), :]
            + taps[kind, 1:2, :] * pre[pl.ds(HALO - 1, length), :]
            + taps[kind, 2:3, :] * pre[pl.ds(HALO, length), :]
        )

    def hidden(zz):
        gathered(zz)
        gate = mix(pre_g, gw, 0, zz)
        value = mix(pre_v, vw, 1, zz)
        act = 0.5 * gate * (1.0 + lax.erf(gate * (0.5**0.5)))
        hid[zz] = (act * value).astype(jnp.bfloat16)

    def wing(h):
        return ds(h * wide, wide, wide)

    def block(zz, cc, h):
        return part.at[zz, ds(cc * rows, rows, rows), wing(h)]

    def rc_copy(zz, cc, h):
        return copy(block(zz, cc, h), rc.at[zz, :, wing(h)], rc_s.at[0], rc_r.at[zz, h], at(cc=cc))

    def zc_copy(way, zz, h):
        ahead = z + 1 - 2 * way
        recv = zc_r.at[jnp.where(zz == ahead, nz * nz + way, zz * nz + h)]
        return copy(block(zz, c, h), zr.at[way, zz, :, wing(h)], zc_s.at[way], recv, at(zz=ahead))

    def zc_wait(way, zz, h):
        await_recv(zr.at[way, zz, :, wing(h)], zc_r.at[zz * nz + h])

    def product(zz, h):
        part[zz, :, wing(h)] = jnp.dot(
            hid[zz], dw[:, wing(h)], preferred_element_type=jnp.float32
        ).astype(jnp.bfloat16)
        for cc in c_others:
            rc_copy(zz, cc, h).start()

    def pair(zz, h):
        for _ in c_others:
            rc_copy(zz, c, h).wait_recv()
            sent = block(zz, c, h)
            sent[...] = (f32(sent) + f32(rc.at[zz, :, wing(h)])).astype(jnp.bfloat16)

    def leave(zz, h):
        @pl.when(ends)
        def _():
            zc_copy(half, zz, h).start()

    def zx_copy(way, zz, h):
        return copy(block(zz, c, h), zx, zc_s.at[way], zc_r.at[nz * nz + 2], at(zz=zz))

    def pass_on(pos, j, e, add=True, skip=False):
        way = jnp.where(z == pos, 0, 1)
        dest = z + j * (1 - 2 * way)
        e = 5 - e if e > 1 else e
        h = e + way * (nz - 1 - 2 * e)

        @pl.when((z == pos) | (z == nz - 1 - pos))
        def _():
            if add:
                zc_wait(way, dest, h)
                sent = block(dest, c, h)
                sent[...] = (f32(sent) + f32(zr.at[way, dest, :, wing(h)])).astype(jnp.bfloat16)
            (zx_copy if skip else zc_copy)(way, dest, h).start()

    def stage(k, turns, now=()):
        h = late(k)
        for i, t in enumerate(turns + [None]):
            if t is not None:
                product(order(t), h)
            if i > 0:
                pair(order(turns[i - 1]), h)
                if turns[i - 1] in now:
                    leave(order(turns[i - 1]), h)

    if nz > 2:
        inner(lambda: relay(2, (0,)))
        hidden(order(2))
        turn(DN, order(0))
        arrive(DN[1:], order(1))
        inner(lambda: relay(2, (1,)))
        hidden(order(1))
        inner(lambda: relay(2, (2,)))
        rest(DN, order(0))
        stage(0, [2, 1], (2, 1))
        turn(DN, order(1))
        arrive(DN, late(2))
        inner(lambda: relay(2, range(3, BITS)))
        rest(DN, order(1))
        stage(1, [2, 1], (2, 1))
        turn(DN, late(2))
        relay(3, range(BITS))
        arrive(DN, late(3))
        hidden(order(3))
        stage(0, [3], (3,))
        stage(1, [3], (3,))
        pass_on(2, 1, 3, add=False)
        pass_on(1, 1, 0)
        pass_on(1, 1, 1)
        rest(DN, late(2))
        stage(2, [3, 2, 1], (3, 2))
        turn(DN, late(3))
        hidden(order(0))
        for k in range(3):
            product(order(0), late(k))
        pass_on(1, 2, 0)
        pass_on(1, 2, 1)
        rest(DN, late(3))
        stage(3, [3, 2, 1], (3, 2))
        leave(order(1), late(2))
        leave(order(1), late(3))
        product(order(0), late(3))
        pass_on(2, 1, 0)
        pass_on(1, 2, 2)
        pass_on(1, 1, 2)
        pass_on(2, 1, 1)
        pass_on(1, 2, 3, skip=True)
        pass_on(2, 1, 2)
        pass_on(1, 1, 3)
        for k in range(nz):
            pair(order(0), order(k))
    else:
        hidden(order(1))
        hidden(order(0))
        turn(DN, order(0))
        rest(DN, order(0))
        stage(0, [1, 0], (1,))
        arrive(DN, order(1))
        turn(DN, order(1))
        rest(DN, order(1))
        stage(1, [1, 0], (1,))

    for way in range(2):
        for p in range(nz - 1):

            @pl.when(place_of(way) == p)
            def _():
                await_send(part.at[pl.ds(0, p + 1), pl.ds(0, rows)], tz_s.at[way])
                await_send(part.at[pl.ds(0, nz - 1 - p), pl.ds(0, rows)], zc_s.at[way])

                @pl.when(keeper)
                def _():
                    await_send(part.at[pl.ds(0, p + 1), pl.ds(0, HALO)], hz_s.at[way])

    @pl.when((c == nc - 1) & (y < ny - 1))
    def _():
        await_send(lead(z), halo_s.at[0])

    if nc > 1:
        others = part.at[:, pl.ds(0, rows * (nc - 1))]
        await_send(others, tc_s.at[0])
        await_send(others, rc_s.at[0])

        @pl.when(keeper)
        def _():
            await_send(part.at[:, pl.ds(0, HALO * (nc - 1))], hc_s.at[0])

    if ny > 1:
        await_send(tap_bulk(), tap_s.at[0])
    for kind in GV + DN:
        for way, (a, b) in enumerate([(nz - 1, 1), (nz * (nx - 1), 1), (nz, ny - 1), (nz * (nx - 1), ny - 1)]):
            if a and b:
                await_send(bulk(kind, a, b), w_s.at[kind, way])

    for way in range(2):
        back = z - 1 + 2 * way

        @pl.when(inside(back))
        def _():
            await_recv(zr.at[way, z], zc_r.at[nz * nz + way])

        @pl.when(jnp.logical_not(inside(back)))
        def _():
            zr[way, z] = jnp.zeros((rows, width), jnp.bfloat16)

    if nz > 2:

        @pl.when(ends)
        def _():
            await_recv(zx, zc_r.at[nz * nz + 2])
            last = zr.at[1 - half, z, :, wing(1 + half)]
            last[...] = (f32(last) + f32(zx)).astype(jnp.bfloat16)

    def finish():
        summed = f32(part.at[z, ds(c * rows, rows, rows)]) + f32(zr.at[0, z]) + f32(zr.at[1, z])
        average = jnp.mean(summed, axis=1, keepdims=True)
        centered = summed - average
        variance = jnp.mean(centered * centered, axis=1, keepdims=True)
        normed = centered * lax.rsqrt(variance + 1e-05) * gain_ref[...] + shift_ref[...]
        out_ref[...] = normed.astype(out_ref.dtype)

    finish()


def solution(mesh):
    n_fs, n_tp = mesh.shape["fs"], mesh.shape["tp"]
    nc = 2 if n_tp % 2 == 0 else 1
    ny = n_tp // nc

    def local(tokens, gate_weight, value_weight, gate_taps, value_taps, down_weight, gain, shift):
        rows, width = tokens.shape
        depth, held = gate_weight.shape
        count = gate_taps.shape[0]
        nz = 4
        while nz > 2 and (n_fs % nz or held % (128 * nz)):
            nz //= 2
        nx = n_fs // nz
        units = held // nz
        cols = down_weight.shape[1]
        length = nc * rows
        bf16 = jnp.bfloat16
        dma = pltpu.SemaphoreType.DMA
        return pl.pallas_call(
            functools.partial(kernel, (nz, nx, ny, nc)),
            out_shape=pltpu.VMEM((rows, width), bf16),
            in_specs=[pl.BlockSpec(memory_space=pltpu.HBM)] * 8,
            out_specs=pl.BlockSpec(memory_space=pltpu.VMEM),
            scratch_shapes=[
                pltpu.VMEM((depth, held), bf16),
                pltpu.VMEM((depth, held), bf16),
                pltpu.VMEM((2, count, held), jnp.float32),
                pltpu.VMEM(down_weight.shape, bf16),
                pltpu.VMEM((1, width), jnp.float32),
                pltpu.VMEM((1, width), jnp.float32),
                dma((9,)),
                pltpu.VMEM((nz, HALO + length, width), bf16),
                pltpu.VMEM((width, ny * units), bf16),
                pltpu.VMEM((width, ny * units), bf16),
                pltpu.VMEM((ny * units, width), bf16),
                pltpu.VMEM((2, count, ny * units), jnp.float32),
                pltpu.VMEM((HALO + length, ny * units), jnp.float32),
                pltpu.VMEM((HALO + length, ny * units), jnp.float32),
                pltpu.VMEM((nz, length, ny * units), bf16),
                pltpu.VMEM((nz, length, width), bf16),
                pltpu.VMEM((nz, rows, width), bf16),
                pltpu.VMEM((2, nz, rows, width), bf16),
                pltpu.VMEM((rows, nx * cols), bf16),
                dma((nz, BITS)),
                dma((nz,)),
                dma((2,)),
                dma((1,)),
                dma((nz,)),
                dma((1,)),
                dma((2,)),
                dma((1,)),
                dma((1,)),
                dma((1,)),
                dma((2, nz)),
                dma((4, nz, max(nx, ny, 2) - 1)),
                dma((2 + 2 * nz,)),
                dma((4, 4)),
                dma((nz, nz)),
                dma((1,)),
                dma((nz * nz + 3,)),
                dma((2,)),
            ],
            compiler_params=pltpu.CompilerParams(
                collective_id=0, has_side_effects=True, vmem_limit_bytes=58 * 2**20
            ),
        )(
            tokens, gate_weight, value_weight, gate_taps, value_taps, down_weight,
            gain.reshape(1, width), shift.reshape(1, width),
        )

    in_specs = (
        P(("fs", "tp"), None),
        P("fs", "tp"),
        P("fs", "tp"),
        P(None, "tp"),
        P(None, "tp"),
        P("tp", "fs"),
        P(),
        P(),
    )
    out_specs = P(("fs", "tp"), None)
    return jax.shard_map(local, mesh=mesh, in_specs=in_specs, out_specs=out_specs, check_vma=False)
```

```python
import functools

import jax
import jax.numpy as jnp
from jax import lax
from jax.experimental import pallas as pl
from jax.experimental.pallas import tpu as pltpu
from jax.sharding import PartitionSpec as P

MESH = pl.DeviceIdType.MESH
HALO = 16
BITS = 4
GV = (0, 1)
DN = (2, 3)


def kernel(
    dims,
    x_hbm, g_hbm, v_hbm, gt_hbm, vt_hbm, d_hbm, gain_hbm, shift_hbm,
    out_ref,
    g_ref, v_ref, tapin, d_ref, gain_ref, shift_ref, in_s,
    tok, gw, vw, dw, taps, pre_g, pre_v, hid, part, rc, zr, zx,
    tok_r, tokc_r, tz_s, tc_s, halo_r, halo_s, hz_s, hc_s, tap_r, tap_s,
    wl_r, wt_r, wr_r, w_s, rc_r, rc_s, zc_r, zc_s,
):
    nz, nx, ny, nc = dims
    rows, width = x_hbm.shape
    depth = g_ref.shape[0]
    units = gw.shape[1] // ny
    cols = d_ref.shape[1]
    length = nc * rows
    bit = rows // BITS
    top = units // 2
    wide = nx * cols
    fs = lax.axis_index("fs")
    tp = lax.axis_index("tp")
    z, x = fs // nx, fs % nx
    y, c = tp // nc, tp % nc

    def at(zz=z, xx=x, yy=y, cc=c):
        return {"fs": zz * nx + xx, "tp": yy * nc + cc}

    z_others = [(z + i) % nz for i in range(1, nz)]
    x_others = [(x + i) % nx for i in range(1, nx)]
    y_others = [(y + i) % ny for i in range(1, ny)]
    c_others = [(c + i) % nc for i in range(1, nc)]

    def ds(start, size, unit):
        return pl.ds(pl.multiple_of(start, unit), size)

    mine = ds(fs * depth, depth, depth)
    here = ds(y * units, units, 128)
    part_units = ds(z * units, units, 128)
    moves = [
        (g_hbm, g_ref, 0),
        (v_hbm, v_ref, 1),
        (x_hbm, tok.at[z, ds(HALO + c * rows, rows, 16)], 2),
        (d_hbm, d_ref, 3),
        (gt_hbm, tapin.at[0], 4),
        (vt_hbm, tapin.at[1], 4),
        (g_hbm.at[:, part_units], gw.at[mine, here], 5),
        (v_hbm.at[:, part_units], vw.at[mine, here], 5),
        (d_hbm.at[ds(z * units, units, 16)], dw.at[ds(y * units, units, 16), ds(fs * cols, cols, cols)], 5),
        (gt_hbm.at[:, part_units], taps.at[0, :, here], 6),
        (vt_hbm.at[:, part_units], taps.at[1, :, here], 6),
        (gain_hbm, gain_ref, 7),
        (shift_hbm, shift_ref, 8),
    ]
    for src, dst, i in moves:
        pltpu.make_async_copy(src, dst, in_s.at[i]).start()

    def loaded(i):
        whole = [
            g_ref, v_ref, slot_z, d_ref, tapin, gw.at[pl.ds(0, 3 * depth), pl.ds(0, units)],
            taps.at[:, :, here], gain_ref, shift_ref,
        ][i]
        pltpu.make_async_copy(whole, whole, in_s.at[i]).wait()

    slot_z = tok.at[z, ds(HALO + c * rows, rows, 16)]

    barrier = pltpu.get_barrier_semaphore()
    partners = (
        [at(zz=i) for i in z_others]
        + [at(xx=i) for i in x_others]
        + [at(yy=i) for i in y_others]
        + [at(cc=i) for i in c_others]
    )
    for partner in partners:
        pl.semaphore_signal(barrier, inc=1, device_id=partner, device_id_type=MESH)
    pl.semaphore_wait(barrier, len(partners))

    def copy(src, dst, send, recv, device):
        return pltpu.make_async_remote_copy(
            src_ref=src, dst_ref=dst, send_sem=send, recv_sem=recv,
            device_id=device, device_id_type=MESH,
        )

    half = (2 * z) // nz
    near = z + half * (nz - 1 - 2 * z)

    def order(j):
        past = (j - near - 1 + nz) // nz
        f = past * j + (1 - past) * (near - j)
        return f + half * (nz - 1 - 2 * f)

    ends = (z == 0) | (z == nz - 1)

    def early(k):
        return jnp.where(ends, order(3 - k), order(k)) if nz > 2 and k in (1, 2) else order(k)

    def late(k):
        return order(5 - k) if nz > 2 and k in (2, 3) else order(k)

    def inside(zz):
        return (zz >= 0) & (zz < nz)

    def inner(act):
        @pl.when(jnp.logical_not(ends))
        def _():
            act()

    def outer(act):
        @pl.when(ends)
        def _():
            act()

    def piece(kind, zz):
        if kind >= 2:
            return d_ref.at[ds(zz * units + (kind - 2) * top, top, 16)]
        ref = g_ref if kind == 0 else v_ref
        return ref.at[:, ds(zz * units, units, 128)]

    def place(kind, src, yy):
        if kind >= 2:
            return dw.at[ds(yy * units + (kind - 2) * top, top, 16), ds(src * cols, cols, cols)]
        ref = gw if kind == 0 else vw
        return ref.at[ds(src * depth, depth, depth), ds(yy * units, units, 128)]

    def bulk(kind, a, b):
        if kind >= 2:
            return dw.at[pl.ds(0, top * b), pl.ds(0, cols * a)]
        return gw.at[pl.ds(0, depth * a), pl.ds(0, units * b)]

    def final(kind, zz):
        return wr_r.at[kind if kind < 2 else 2 + (kind - 2) * nz + zz]

    def await_recv(ref, sem):
        copy(ref, ref, w_s.at[0, 0], sem, partners[0]).wait_recv()

    def await_send(ref, sem):
        copy(ref, ref, sem, wl_r.at[0, 0], partners[0]).wait_send()

    def w_z(kind, zz):
        return copy(piece(kind, zz), place(kind, fs, y), w_s.at[kind, 0], wl_r.at[kind // 2, z], at(zz=zz))

    def spread(kind, src, zz):
        dst = place(kind, zz * nx + x, y)
        for i, xx in enumerate(x_others):
            recv = wt_r.at[kind, zz, nx - i - 2] if kind % 2 == 0 else final(kind, zz)
            copy(src, dst, w_s.at[kind, 1], recv, at(xx=xx)).start()
        for i, yy in enumerate(y_others):
            recv = wt_r.at[kind, zz, ny - i - 2] if kind % 2 == 1 else final(kind, zz)
            copy(src, dst, w_s.at[kind, 2], recv, at(yy=yy)).start()

    def own(kinds):
        for kind in kinds:
            spread(kind, piece(kind, z), z)

    def arrive(kinds, zz):
        for kind in kinds:
            if kind % 2 == 0:
                await_recv(bulk(kind, 2, 1) if kind < 2 else bulk(kind, 1, 2), wl_r.at[kind // 2, zz])
            spread(kind, place(kind, zz * nx + x, y), zz)

    def turn(kinds, zz):
        for kind in kinds:
            across, along = (x_others, y_others) if kind % 2 == 0 else (y_others, x_others)
            for i, a in enumerate(across):
                ref = place(kind, zz * nx + a, y) if kind % 2 == 0 else place(kind, zz * nx + x, a)
                await_recv(ref, wt_r.at[kind, zz, i])
                for b in along:
                    device = at(yy=b) if kind % 2 == 0 else at(xx=b)
                    copy(ref, ref, w_s.at[kind, 3], final(kind, zz), device).start()

    def rest(kinds, zz):
        for kind in kinds:
            a = nx if kind % 2 == 0 else nx - 1
            b = ny - 1 if kind % 2 == 0 else ny
            if a and b:
                await_recv(bulk(kind, a * nz if kind < 2 else a, b), final(kind, zz))

    def slot(zz, cc):
        return tok.at[zz, ds(HALO + cc * rows, rows, 16)]

    def chunk(zz, cc, b):
        return tok.at[zz, ds(HALO + cc * rows + b * bit, bit, 16)]

    def tok_z(src, zz, way, b):
        return copy(src, chunk(zz, c, b), tz_s.at[way], tok_r.at[zz, b], at(zz=z + 1 - 2 * way))

    def tok_c(src, zz, cc):
        return copy(src, slot(zz, c), tc_s.at[0], tokc_r.at[zz], at(cc=cc))

    keeper = (c == nc - 1) & (y > 0)

    def lead(zz):
        return tok.at[zz, pl.ds(0, HALO)]

    def halo_y():
        return copy(tok.at[z, ds(c * rows + rows, HALO, 16)], lead(z), halo_s.at[0], halo_r.at[z], at(yy=y + 1))

    def halo_z(zz, way):
        return copy(lead(zz), lead(zz), hz_s.at[way], halo_r.at[zz], at(zz=z + 1 - 2 * way))

    def halo_c(zz, cc):
        return copy(lead(zz), lead(zz), hc_s.at[0], halo_r.at[zz], at(cc=cc))

    def halo_wait(zz):
        await_recv(lead(zz), halo_r.at[zz])

    def keep(zz, ways, further):
        @pl.when(keeper)
        def _():
            halo_wait(zz)
            if further:
                for way in ways:

                    @pl.when(inside(z + 1 - 2 * way))
                    def _():
                        halo_z(zz, way).start()

            for cc in c_others:
                halo_c(zz, cc).start()

    def cross(src, zz):
        for cc in c_others:
            tok_c(src, zz, cc).start()

    def relay(step, bits):
        for way in (half, 1 - half):
            zz = z - step + 2 * step * way
            ahead = z + 1 - 2 * way

            @pl.when(inside(zz))
            def _():
                for b in bits:
                    await_recv(chunk(zz, c, b), tok_r.at[zz, b])
                    if step < nz - 1:

                        @pl.when(inside(ahead))
                        def _():
                            tok_z(chunk(zz, c, b), zz, way, b).start()

                    for cc in c_others:
                        copy(chunk(zz, c, b), chunk(zz, c, b), tc_s.at[0], tokc_r.at[zz], at(cc=cc)).start()

                if bits[-1] == BITS - 1:
                    keep(zz, (way,), step < nz - 1)

    def gathered(zz):
        for cc in c_others:
            await_recv(slot(zz, cc), tokc_r.at[zz])

        @pl.when((y > 0) & (c < nc - 1))
        def _():
            halo_wait(zz)

    def tap(kind, yy):
        return copy(tapin.at[kind, :, part_units], taps.at[kind, :, here], tap_s.at[0], tap_r.at[0], at(yy=yy))

    def tap_bulk():
        return taps.at[:, :, pl.ds(0, units * (ny - 1))]

    def place_of(way):
        return z + way * (nz - 1 - 2 * z)

    def line(kinds, way, steps, wanted=True):
        for step in steps:
            zz = z + step * (1 - 2 * way)

            @pl.when(inside(zz) & wanted)
            def _():
                for kind in kinds:
                    w_z(kind, zz).start()

    central = nz // 2 - 1

    loaded(0)
    loaded(1)
    own(GV)
    for way in range(2):
        pos = place_of(way)
        line(GV, way, (1,), pos == 0)
        line(GV, way, range(nz - 1, 0, -1), pos > 0)
    loaded(2)

    @pl.when((c == nc - 1) & (y < ny - 1))
    def _():
        halo_y().start()

    for way in range(2):
        pos = place_of(way)

        @pl.when(inside(z + 1 - 2 * way))
        def _():
            for b in range(BITS):
                tok_z(chunk(z, c, b), z, way, b).start()

        line(GV, way, range(nz - 1, 1, -1), pos == 0)
    loaded(3)
    loaded(4)
    for way in range(2):
        line(DN, way, (1,), place_of(way) != central)
    for kind in range(2):
        for yy in y_others:
            tap(kind, yy).start()
    cross(slot(z, c), z)

    @pl.when(y == 0)
    def _():
        tok[:, 0:HALO, :] = jnp.zeros((nz, HALO, width), jnp.bfloat16)

    keep(z, range(2), True)
    side = nz // 2
    for k in range(1, nz):
        first = k in (1, nz - 1)
        if first:
            turn(GV, early(k - 1))
        arrive(GV, early(k))
        if not first:
            turn(GV, early(k - 1))
    relay(1, range(BITS))
    for way in range(2):
        line(DN, way, range(1, nz), place_of(way) == central)
    turn(GV, order(nz - 1))
    own(DN)
    for way in range(2):
        line(DN, way, range(2, nz), place_of(way) < central)
    if nz > 2:
        arrive(DN[:1], order(1))
        outer(lambda: relay(2, range(BITS)))
    for i in range(5, 9):
        loaded(i)
    if ny > 1:
        await_recv(tap_bulk(), tap_r.at[0])
    rest(GV, 0)

    def f32(ref):
        return ref[...].astype(jnp.float32)

    def mix(pre, w, kind, zz):
        raw = jnp.dot(tok[zz], w[...], preferred_element_type=jnp.float32)
        pre[...] = raw.astype(jnp.bfloat16).astype(jnp.float32)
        return (
            taps[kind, 0:1, :] * pre[pl.ds(HALO - 2, length), :]
            + taps[kind, 1:2, :] * pre[pl.ds(HALO - 1, length), :]
            + taps[kind, 2:3, :] * pre[pl.ds(HALO, length), :]
        )

    def hidden(zz):
        gathered(zz)
        gate = mix(pre_g, gw, 0, zz)
        value = mix(pre_v, vw, 1, zz)
        act = 0.5 * gate * (1.0 + lax.erf(gate * (0.5**0.5)))
        hid[zz] = (act * value).astype(jnp.bfloat16)

    def wing(h):
        return ds(h * wide, wide, wide)

    def block(zz, cc, h):
        return part.at[zz, ds(cc * rows, rows, rows), wing(h)]

    def rc_copy(zz, cc, h):
        return copy(block(zz, cc, h), rc.at[zz, :, wing(h)], rc_s.at[0], rc_r.at[zz, h], at(cc=cc))

    def zc_copy(way, zz, h):
        ahead = z + 1 - 2 * way
        recv = zc_r.at[jnp.where(zz == ahead, nz * nz + way, zz * nz + h)]
        return copy(block(zz, c, h), zr.at[way, zz, :, wing(h)], zc_s.at[way], recv, at(zz=ahead))

    def zc_wait(way, zz, h):
        await_recv(zr.at[way, zz, :, wing(h)], zc_r.at[zz * nz + h])

    def product(zz, h):
        part[zz, :, wing(h)] = jnp.dot(
            hid[zz], dw[:, wing(h)], preferred_element_type=jnp.float32
        ).astype(jnp.bfloat16)
        for cc in c_others:
            rc_copy(zz, cc, h).start()

    def pair(zz, h):
        for _ in c_others:
            rc_copy(zz, c, h).wait_recv()
            sent = block(zz, c, h)
            sent[...] = (f32(sent) + f32(rc.at[zz, :, wing(h)])).astype(jnp.bfloat16)

    def leave(zz, h):
        @pl.when(ends)
        def _():
            zc_copy(half, zz, h).start()

    def zx_copy(way, zz, h):
        return copy(block(zz, c, h), zx, zc_s.at[way], zc_r.at[nz * nz + 2], at(zz=zz))

    def pass_on(pos, j, e, add=True, skip=False):
        way = jnp.where(z == pos, 0, 1)
        dest = z + j * (1 - 2 * way)
        e = 5 - e if e > 1 else e
        h = e + way * (nz - 1 - 2 * e)

        @pl.when((z == pos) | (z == nz - 1 - pos))
        def _():
            if add:
                zc_wait(way, dest, h)
                sent = block(dest, c, h)
                sent[...] = (f32(sent) + f32(zr.at[way, dest, :, wing(h)])).astype(jnp.bfloat16)
            (zx_copy if skip else zc_copy)(way, dest, h).start()

    def stage(k, turns, now=()):
        h = late(k)
        for i, t in enumerate(turns + [None]):
            if t is not None:
                product(order(t), h)
            if i > 0:
                pair(order(turns[i - 1]), h)
                if turns[i - 1] in now:
                    leave(order(turns[i - 1]), h)

    if nz > 2:
        inner(lambda: relay(2, (0,)))
        hidden(order(2))
        turn(DN, order(0))
        arrive(DN[1:], order(1))
        inner(lambda: relay(2, (1,)))
        hidden(order(1))
        inner(lambda: relay(2, (2,)))
        rest(DN, order(0))
        stage(0, [2, 1], (2, 1))
        turn(DN, order(1))
        arrive(DN, late(2))
        inner(lambda: relay(2, range(3, BITS)))
        rest(DN, order(1))
        stage(1, [2, 1], (2, 1))
        turn(DN, late(2))
        relay(3, range(BITS))
        arrive(DN, late(3))
        hidden(order(3))
        for k in range(2):
            product(order(3), late(k))
        for k in range(2):
            pair(order(3), late(k))
            leave(order(3), late(k))
        pass_on(2, 1, 3, add=False)
        pass_on(1, 1, 0)
        pass_on(1, 1, 1)
        rest(DN, late(2))
        stage(2, [3, 2, 1], (3, 2))
        turn(DN, late(3))
        hidden(order(0))
        for k in range(3):
            product(order(0), late(k))
        pass_on(1, 2, 0)
        pass_on(1, 2, 1)
        rest(DN, late(3))
        stage(3, [3, 2, 1], (3, 2))
        leave(order(1), late(2))
        leave(order(1), late(3))
        product(order(0), late(3))
        pass_on(2, 1, 0)
        pass_on(1, 2, 2)
        pass_on(1, 1, 2)
        pass_on(2, 1, 1)
        pass_on(1, 2, 3, skip=True)
        pass_on(2, 1, 2)
        pass_on(1, 1, 3)
        for k in range(nz):
            pair(order(0), order(k))
    else:
        hidden(order(1))
        hidden(order(0))
        turn(DN, order(0))
        rest(DN, order(0))
        stage(0, [1, 0], (1,))
        arrive(DN, order(1))
        turn(DN, order(1))
        rest(DN, order(1))
        stage(1, [1, 0], (1,))

    for way in range(2):
        for p in range(nz - 1):

            @pl.when(place_of(way) == p)
            def _():
                await_send(part.at[pl.ds(0, p + 1), pl.ds(0, rows)], tz_s.at[way])
                await_send(part.at[pl.ds(0, nz - 1 - p), pl.ds(0, rows)], zc_s.at[way])

                @pl.when(keeper)
                def _():
                    await_send(part.at[pl.ds(0, p + 1), pl.ds(0, HALO)], hz_s.at[way])

    @pl.when((c == nc - 1) & (y < ny - 1))
    def _():
        await_send(lead(z), halo_s.at[0])

    if nc > 1:
        others = part.at[:, pl.ds(0, rows * (nc - 1))]
        await_send(others, tc_s.at[0])
        await_send(others, rc_s.at[0])

        @pl.when(keeper)
        def _():
            await_send(part.at[:, pl.ds(0, HALO * (nc - 1))], hc_s.at[0])

    if ny > 1:
        await_send(tap_bulk(), tap_s.at[0])
    for kind in GV + DN:
        for way, (a, b) in enumerate([(nz - 1, 1), (nz * (nx - 1), 1), (nz, ny - 1), (nz * (nx - 1), ny - 1)]):
            if a and b:
                await_send(bulk(kind, a, b), w_s.at[kind, way])

    for way in range(2):
        back = z - 1 + 2 * way

        @pl.when(inside(back))
        def _():
            await_recv(zr.at[way, z], zc_r.at[nz * nz + way])

        @pl.when(jnp.logical_not(inside(back)))
        def _():
            zr[way, z] = jnp.zeros((rows, width), jnp.bfloat16)

    if nz > 2:

        @pl.when(ends)
        def _():
            await_recv(zx, zc_r.at[nz * nz + 2])
            last = zr.at[1 - half, z, :, wing(1 + half)]
            last[...] = (f32(last) + f32(zx)).astype(jnp.bfloat16)

    def finish():
        summed = f32(part.at[z, ds(c * rows, rows, rows)]) + f32(zr.at[0, z]) + f32(zr.at[1, z])
        average = jnp.mean(summed, axis=1, keepdims=True)
        centered = summed - average
        variance = jnp.mean(centered * centered, axis=1, keepdims=True)
        normed = centered * lax.rsqrt(variance + 1e-05) * gain_ref[...] + shift_ref[...]
        out_ref[...] = normed.astype(out_ref.dtype)

    finish()


def solution(mesh):
    n_fs, n_tp = mesh.shape["fs"], mesh.shape["tp"]
    nc = 2 if n_tp % 2 == 0 else 1
    ny = n_tp // nc

    def local(tokens, gate_weight, value_weight, gate_taps, value_taps, down_weight, gain, shift):
        rows, width = tokens.shape
        depth, held = gate_weight.shape
        count = gate_taps.shape[0]
        nz = 4
        while nz > 2 and (n_fs % nz or held % (128 * nz)):
            nz //= 2
        nx = n_fs // nz
        units = held // nz
        cols = down_weight.shape[1]
        length = nc * rows
        bf16 = jnp.bfloat16
        dma = pltpu.SemaphoreType.DMA
        return pl.pallas_call(
            functools.partial(kernel, (nz, nx, ny, nc)),
            out_shape=pltpu.VMEM((rows, width), bf16),
            in_specs=[pl.BlockSpec(memory_space=pltpu.HBM)] * 8,
            out_specs=pl.BlockSpec(memory_space=pltpu.VMEM),
            scratch_shapes=[
                pltpu.VMEM((depth, held), bf16),
                pltpu.VMEM((depth, held), bf16),
                pltpu.VMEM((2, count, held), jnp.float32),
                pltpu.VMEM(down_weight.shape, bf16),
                pltpu.VMEM((1, width), jnp.float32),
                pltpu.VMEM((1, width), jnp.float32),
                dma((9,)),
                pltpu.VMEM((nz, HALO + length, width), bf16),
                pltpu.VMEM((width, ny * units), bf16),
                pltpu.VMEM((width, ny * units), bf16),
                pltpu.VMEM((ny * units, width), bf16),
                pltpu.VMEM((2, count, ny * units), jnp.float32),
                pltpu.VMEM((HALO + length, ny * units), jnp.float32),
                pltpu.VMEM((HALO + length, ny * units), jnp.float32),
                pltpu.VMEM((nz, length, ny * units), bf16),
                pltpu.VMEM((nz, length, width), bf16),
                pltpu.VMEM((nz, rows, width), bf16),
                pltpu.VMEM((2, nz, rows, width), bf16),
                pltpu.VMEM((rows, nx * cols), bf16),
                dma((nz, BITS)),
                dma((nz,)),
                dma((2,)),
                dma((1,)),
                dma((nz,)),
                dma((1,)),
                dma((2,)),
                dma((1,)),
                dma((1,)),
                dma((1,)),
                dma((2, nz)),
                dma((4, nz, max(nx, ny, 2) - 1)),
                dma((2 + 2 * nz,)),
                dma((4, 4)),
                dma((nz, nz)),
                dma((1,)),
                dma((nz * nz + 3,)),
                dma((2,)),
            ],
            compiler_params=pltpu.CompilerParams(
                collective_id=0, has_side_effects=True, vmem_limit_bytes=58 * 2**20
            ),
        )(
            tokens, gate_weight, value_weight, gate_taps, value_taps, down_weight,
            gain.reshape(1, width), shift.reshape(1, width),
        )

    in_specs = (
        P(("fs", "tp"), None),
        P("fs", "tp"),
        P("fs", "tp"),
        P(None, "tp"),
        P(None, "tp"),
        P("tp", "fs"),
        P(),
        P(),
    )
    out_specs = P(("fs", "tp"), None)
    return jax.shard_map(local, mesh=mesh, in_specs=in_specs, out_specs=out_specs, check_vma=False)
```
